32 devices in a mesh: sp: 8 (over z, x), tp: 4 (over y, core).
Axes of the slice: x: 2, y: 2, z: 4, core: 2. Of those that a mesh axis runs over, the one named last changes fastest.
Arguments:
- mid_state: bfloat16 [2048, 2048], P('sp'), may hold values from -6 to 6
- conv_pre: bfloat16 [2048, 1024], P('sp', 'tp'), may hold values from -8 to 8
- conv_taps: bfloat16 [31, 1024], P(None, 'tp'), may hold values from -1 to 1
- out_proj: bfloat16 [1024, 2048], P('tp'), may hold values from -0.1875 to 0.1875
- route_expert: int32 [2048, 2], P('sp'), may hold values from 0 to 7, as said below
- route_weight: float32 [2048, 2], P('sp'), may hold values from 0.1 to 1
- gate_w: bfloat16 [8, 2048, 2048], P('sp', None, 'tp'), may hold values from -0.125 to 0.125
- up_w: bfloat16 [8, 2048, 2048], P('sp', None, 'tp'), may hold values from -0.125 to 0.125
- down_w: bfloat16 [8, 2048, 2048], P('sp', 'tp'), may hold values from -0.125 to 0.125
- cotangent: bfloat16 [2048, 2048], P('sp'), may hold values from -6 to 6
Outputs:
- grad_gate: bfloat16 [8, 2048, 2048], P('sp', None, 'tp')
- grad_up: bfloat16 [8, 2048, 2048], P('sp', None, 'tp')
- grad_down: bfloat16 [8, 2048, 2048], P('sp', 'tp')
- grad_proj: float32 [2048, 1024], P('sp', 'tp')
- conv_input_grad: float32 [2048, 1024], P('sp', 'tp')
The draws below stay inside these ranges and needn't reach their ends.
Inputs may be any that keep to these rules, and one draw needn't show every extreme that they name: `route_expert`: the two experts of a token are different and lie in one group of 8 // 4 consecutive experts; in every draw some expert is named by more than 68 routes of every aligned block of 256 tokens.
All inputs are finite; a program needn't handle non-finite values.
Results may differ from the reference program's by a relative error of at most 0.02.
Values may be sent and summed in bfloat16 or wider, within the bound.
A program may use at most 128 MiB of HBM per device.

```python
import jax
import jax.numpy as jnp
from jax import lax

D = 2048
FF = 2048
CONV = 1024
KERNEL = 31
TOP = 2
GROUPS = 4
TOK_DEV = 256
TOKENS = 2048
EXPERTS = 8
SLOTS = 68
N_TP = 4


def draw_route_expert(key, part):
    keys = jax.random.split(jax.random.fold_in(key, 17), 6)
    per_group = EXPERTS // GROUPS
    group_pick = jax.random.randint(keys[0], (TOKENS,), 0, GROUPS)
    first_pick = jax.random.randint(keys[1], (TOKENS,), 0, per_group)
    offset_pick = jax.random.randint(keys[2], (TOKENS,), 0, per_group - 1)
    second_pick = (first_pick + 1 + offset_pick) % per_group
    focus = jax.random.randint(keys[3], (), 0, EXPERTS)
    block_shift = jax.random.randint(keys[4], (TOKENS // TOK_DEV,), 0, TOK_DEV)
    row_ids = jnp.arange(TOKENS, dtype=jnp.int32)
    inside = (row_ids % TOK_DEV - block_shift[row_ids // TOK_DEV]) % TOK_DEV
    forced = inside <= SLOTS
    group_pick = jnp.where(forced, focus // per_group, group_pick)
    first_pick = jnp.where(forced, focus % per_group, first_pick)
    second_pick = jnp.where(forced, (focus % per_group + 1 + offset_pick) % per_group, second_pick)
    return jnp.stack([group_pick * per_group + first_pick, group_pick * per_group + second_pick], axis=1).astype(jnp.int32)


def with_spikes(result, own_key, source, target, blocks, factor):
    owner, partner = [(jnp.arange(result.shape[position]) // (result.shape[position] // blocks)).reshape([-1 if axis == position else 1 for axis in range(result.ndim)]) for position in (source, target)]
    chosen = jax.random.permutation(own_key, blocks)[partner]
    strong = (owner == chosen) | (owner == (partner + blocks // 2) % blocks)
    return jnp.where(strong, factor * result, result)


def levels(stream_key, shape, cuts, smallest, top_value):
    def one(axis_at, shards_of):
        steps = jax.random.uniform(jax.random.fold_in(jax.random.fold_in(stream_key, 6), axis_at), (shards_of,), jnp.float32, smallest / len(cuts), top_value / len(cuts))
        return jnp.repeat(jnp.exp(steps), shape[axis_at] // shards_of).reshape((-1,) + (1,) * (len(shape) - axis_at - 1))

    gain = one(*cuts[0])
    for cut in cuts[1:]:
        gain = gain * one(*cut)
    return gain


def bell_draw(rng, extent, scale, bound, pieces=(), kind=jnp.bfloat16):
    values = jax.random.normal(rng, extent, jnp.float32) * scale
    if len(pieces) > 0:
        values = levels(rng, extent, pieces, -0.22, 0.18) * values
    return jnp.clip(values, min=-bound, max=bound).astype(kind)


def heavy_noise(stream_key, shape, deviation, most, cuts, heavy, held_as=jnp.bfloat16):
    array = deviation * jax.random.normal(stream_key, shape, jnp.float32)
    if cuts:
        array = array * levels(stream_key, shape, cuts, -0.22, 0.18)
    return jnp.clip(with_spikes(array, jax.random.fold_in(stream_key, 3), *heavy), -most, most).astype(held_as)


def setup_inputs(seed: int = 0) -> dict:
    key_list = jax.random.split(jax.random.key(seed), 11)
    mid_state = bell_draw(key_list[0], (TOKENS, D), 1.0, 6.0, ((0, 8),))
    conv_pre = bell_draw(key_list[1], (TOKENS, CONV), 1.5, 8.0, ((0, 8), (1, 4)))
    conv_taps = bell_draw(key_list[2], (KERNEL, CONV), KERNEL ** -0.5, 1.0, ((1, 4),))
    out_proj = bell_draw(key_list[3], (CONV, D), CONV ** -0.5, 0.1875, ((0, 4),))
    route_expert = draw_route_expert(jax.random.fold_in(key_list[10], 71), 0)
    route_weight = jnp.clip(0.1 + 0.9 * jax.random.uniform(key_list[5], (TOKENS, TOP), jnp.float32) ** levels(key_list[5], (TOKENS, TOP), ((0, 8),), -0.2, 0.2), 0.1, 1.0)
    gate_w = bell_draw(key_list[6], (EXPERTS, D, FF), D ** -0.5, 0.125, ((0, 8), (2, 4)))
    up_w = bell_draw(key_list[7], (EXPERTS, D, FF), D ** -0.5, 0.125, ((0, 8), (2, 4)))
    down_w = bell_draw(key_list[8], (EXPERTS, FF, D), FF ** -0.5, 0.125, ((0, 8), (1, 4)))
    cotangent = heavy_noise(key_list[9], (TOKENS, D), 1.0, 6.0, ((0, 8),), (0, 1, 8, 2.0))
    return {"mid_state": mid_state, "conv_pre": conv_pre, "conv_taps": conv_taps, "out_proj": out_proj, "route_expert": route_expert, "route_weight": route_weight, "gate_w": gate_w, "up_w": up_w, "down_w": down_w, "cotangent": cotangent}


def silu_slope(value):
    sig = jax.nn.sigmoid(value)
    return sig * (1.0 + value * (1.0 - sig))


def expert_backward(packed):
    inputs, seeds, gate_mat, up_mat, down_mat = packed
    gate_pre = jnp.dot(inputs, gate_mat, preferred_element_type=jnp.float32)
    up_pre = jnp.dot(inputs, up_mat, preferred_element_type=jnp.float32)
    gate_act = jax.nn.silu(gate_pre)
    hidden = (gate_act * up_pre).astype(jnp.bfloat16)
    grad_down = jnp.dot(hidden.T, seeds, preferred_element_type=jnp.float32).astype(jnp.bfloat16)
    hidden_grad = jnp.dot(seeds, down_mat.T, preferred_element_type=jnp.float32)
    gate_grad = (hidden_grad * up_pre * silu_slope(gate_pre)).astype(jnp.bfloat16)
    up_grad = (hidden_grad * gate_act).astype(jnp.bfloat16)
    grad_gate = jnp.dot(inputs.T, gate_grad, preferred_element_type=jnp.float32).astype(jnp.bfloat16)
    grad_up = jnp.dot(inputs.T, up_grad, preferred_element_type=jnp.float32).astype(jnp.bfloat16)
    slot_total = inputs.shape[0]
    block_width = FF // N_TP
    gate_blocks = gate_grad.astype(jnp.float32).reshape(slot_total, N_TP, block_width)
    up_blocks = up_grad.astype(jnp.float32).reshape(slot_total, N_TP, block_width)
    gate_wblocks = gate_mat.astype(jnp.float32).reshape(D, N_TP, block_width)
    up_wblocks = up_mat.astype(jnp.float32).reshape(D, N_TP, block_width)
    partial_value = jnp.einsum("rjf,djf->rjd", gate_blocks, gate_wblocks) + jnp.einsum("rjf,djf->rjd", up_blocks, up_wblocks)
    partial_value = partial_value.astype(jnp.bfloat16).astype(jnp.float32)
    input_grad = jnp.sum(partial_value, axis=1).astype(jnp.bfloat16)
    return grad_gate, grad_up, grad_down, input_grad


def reference(mid_state, conv_pre, conv_taps, out_proj, route_expert, route_weight, gate_w, up_w, down_w, cotangent):
    blocks = TOKENS // TOK_DEV
    flat_routes = route_expert.reshape(-1)
    one_hot_table = (flat_routes[:, None] == jnp.arange(EXPERTS, dtype=jnp.int32)[None, :]).astype(jnp.int32)
    one_hot_table = one_hot_table.reshape(blocks, TOK_DEV * TOP, EXPERTS)
    slot_rank = (jnp.sum(jnp.cumsum(one_hot_table, axis=1) * one_hot_table, axis=2) - 1).reshape(-1)
    route_ids = jnp.arange(TOKENS * TOP, dtype=jnp.int32)
    source_block = route_ids // (TOK_DEV * TOP)
    token_ids = route_ids // TOP
    kept_mask = slot_rank < SLOTS
    per_expert = blocks * SLOTS
    slot_index = jnp.where(kept_mask, flat_routes * per_expert + source_block * SLOTS + slot_rank, EXPERTS * per_expert).astype(jnp.int32)
    route_cot = (route_weight.reshape(-1)[:, None] * cotangent[token_ids].astype(jnp.float32)).astype(jnp.bfloat16)
    slot_inputs = jnp.zeros((EXPERTS * per_expert, D), jnp.bfloat16).at[slot_index].set(mid_state[token_ids], mode="drop")
    slot_seeds = jnp.zeros((EXPERTS * per_expert, D), jnp.bfloat16).at[slot_index].set(route_cot, mode="drop")
    grad_gate, grad_up, grad_down, input_grad = lax.map(expert_backward, (slot_inputs.reshape(EXPERTS, per_expert, D), slot_seeds.reshape(EXPERTS, per_expert, D), gate_w, up_w, down_w))
    input_flat = input_grad.reshape(EXPERTS * per_expert, D)
    safe_index = jnp.minimum(slot_index, EXPERTS * per_expert - 1)
    returned = jnp.where(kept_mask[:, None], input_flat[safe_index].astype(jnp.float32), jnp.float32(0.0))
    moe_grad = jnp.sum(returned.reshape(TOKENS, TOP, D), axis=1)
    mid_grad = (cotangent.astype(jnp.float32) + moe_grad).astype(jnp.bfloat16)
    pre_float = conv_pre.astype(jnp.float32)
    activated = jax.nn.silu(pre_float).astype(jnp.bfloat16)
    grad_proj = jnp.dot(mid_grad.T, activated, preferred_element_type=jnp.float32)
    mixed_grad = jnp.dot(mid_grad, out_proj.T, preferred_element_type=jnp.float32)
    conv_grad = (mixed_grad * silu_slope(pre_float)).astype(jnp.bfloat16)
    extended = jnp.concatenate([conv_grad.astype(jnp.float32), jnp.zeros((KERNEL - 1, CONV), jnp.float32)], axis=0)
    conv_input_grad = jnp.zeros((TOKENS, CONV), jnp.float32)
    for lag_index in range(KERNEL):
        conv_input_grad = conv_input_grad + conv_taps[lag_index].astype(jnp.float32)[None, :] * extended[lag_index:lag_index + TOKENS]
    return grad_gate, grad_up, grad_down, grad_proj, conv_input_grad
```

```python
import jax
import jax.numpy as jnp
from jax import lax
from jax.experimental import pallas as pl
from jax.experimental.pallas import tpu as pltpu
from jax.sharding import PartitionSpec as P

D = 2048
KERNEL = 31
TOP = 2
GROUPS = 4
MESH = pl.DeviceIdType.MESH


def passed_along(value, axis, steps):
    count = lax.axis_size(axis)
    initial, last = (max(0, -steps), min(count, count - steps))
    return lax.ppermute(value, axis, [(source, source + steps) for source in range(initial, last)])


def silu_slope(value):
    sig = jax.nn.sigmoid(value)
    return sig * (1.0 + value * (1.0 - sig))


def body(
    mid_state,
    conv_pre,
    conv_taps,
    out_proj,
    route_expert,
    route_weight,
    gate_w,
    up_w,
    down_w,
    cotangent,
):
    groups = lax.axis_size("sp")
    token_count = mid_state.shape[0]
    slot_count = 17 * token_count * TOP // (16 * groups)
    flat_routes = route_expert.reshape(-1)
    one_hot_table = (flat_routes[:, None] == jnp.arange(groups, dtype=jnp.int32)[None, :]).astype(
        jnp.int32
    )
    slot_rank = jnp.sum(jnp.cumsum(one_hot_table, axis=0) * one_hot_table, axis=1) - 1
    kept_mask = slot_rank < slot_count
    slot_index = jnp.where(kept_mask, flat_routes * slot_count + slot_rank, groups * slot_count)
    token_ids = jnp.arange(token_count * TOP, dtype=jnp.int32) // TOP
    route_cot = (
        route_weight.reshape(-1)[:, None] * cotangent[token_ids].astype(jnp.float32)
    ).astype(jnp.bfloat16)
    send_inputs = (
        jnp.zeros((groups * slot_count, D), jnp.bfloat16)
        .at[slot_index]
        .set(mid_state[token_ids], mode="drop")
        .reshape(groups, slot_count, D)
    )
    send_seeds = (
        jnp.zeros((groups * slot_count, D), jnp.bfloat16)
        .at[slot_index]
        .set(route_cot, mode="drop")
        .reshape(groups, slot_count, D)
    )
    got_inputs, got_seeds = (
        lax.all_to_all(send_inputs, "sp", split_axis=0, concat_axis=0, tiled=True),
        lax.all_to_all(send_seeds, "sp", split_axis=0, concat_axis=0, tiled=True),
    )
    inputs = got_inputs.reshape(groups * slot_count, D)
    seeds = got_seeds.reshape(groups * slot_count, D)
    gate_mat = gate_w[0]
    up_mat = up_w[0]
    down_mat = down_w[0]
    gate_pre = jnp.dot(inputs, gate_mat, preferred_element_type=jnp.float32)
    up_pre = jnp.dot(inputs, up_mat, preferred_element_type=jnp.float32)
    gate_act = jax.nn.silu(gate_pre)
    hidden = (gate_act * up_pre).astype(jnp.bfloat16)
    hidden_grad = lax.dot_general(
        seeds, down_mat, (((1,), (1,)), ((), ())), preferred_element_type=jnp.float32
    )
    gate_grad = (hidden_grad * up_pre * silu_slope(gate_pre)).astype(jnp.bfloat16)
    up_grad = (hidden_grad * gate_act).astype(jnp.bfloat16)
    grad_down = lax.dot_general(
        hidden, seeds, (((0,), (0,)), ((), ())), preferred_element_type=jnp.float32
    ).astype(jnp.bfloat16)
    grad_gate = lax.dot_general(
        inputs, gate_grad, (((0,), (0,)), ((), ())), preferred_element_type=jnp.float32
    ).astype(jnp.bfloat16)
    grad_up = lax.dot_general(
        inputs, up_grad, (((0,), (0,)), ((), ())), preferred_element_type=jnp.float32
    ).astype(jnp.bfloat16)
    weight_results = (grad_gate, grad_up, grad_down)
    partial_value = lax.dot_general(
        gate_grad, gate_mat, (((1,), (1,)), ((), ())), preferred_element_type=jnp.float32
    )
    partial_value = partial_value + lax.dot_general(
        up_grad, up_mat, (((1,), (1,)), ((), ())), preferred_element_type=jnp.float32
    )
    partial_value = partial_value.astype(jnp.bfloat16).astype(jnp.float32)
    safe_index = jnp.minimum(slot_index, groups * slot_count - 1)
    slice_width = D // lax.axis_size("tp")
    summed = lax.psum_scatter(
        partial_value.astype(jnp.bfloat16), "tp", scatter_dimension=1, tiled=True
    )
    returned = lax.all_to_all(
        summed.reshape(groups, slot_count, slice_width),
        "sp",
        split_axis=0,
        concat_axis=0,
        tiled=True,
    ).reshape(groups * slot_count, slice_width)
    picked = jnp.where(
        kept_mask[:, None], returned[safe_index].astype(jnp.float32), jnp.float32(0.0)
    )
    moe_grad = jnp.sum(picked.reshape(token_count, TOP, slice_width), axis=1)
    own_cot = lax.dynamic_slice_in_dim(
        cotangent, lax.axis_index("tp") * slice_width, slice_width, 1
    )
    mid_part = (own_cot.astype(jnp.float32) + moe_grad).astype(jnp.bfloat16)
    mid_grad = lax.all_gather(mid_part, "tp", axis=1, tiled=True)
    grad_gate, grad_up, grad_down = weight_results
    pre_float = conv_pre.astype(jnp.float32)
    activated = jax.nn.silu(pre_float).astype(jnp.bfloat16)
    mixed_grad = lax.dot_general(
        mid_grad, out_proj, (((1,), (1,)), ((), ())), preferred_element_type=jnp.float32
    )
    conv_grad = (mixed_grad * silu_slope(pre_float)).astype(jnp.bfloat16)
    next_head = passed_along(conv_grad[: KERNEL - 1], "sp", -1)
    extended = jnp.concatenate([conv_grad, next_head], axis=0).astype(jnp.float32)
    conv_input_grad = jnp.zeros(conv_grad.shape, jnp.float32)
    for lag_index in range(KERNEL):
        conv_input_grad = (
            conv_input_grad
            + conv_taps[lag_index].astype(jnp.float32)[None, :]
            * extended[lag_index : lag_index + token_count]
        )
    grad_proj = lax.psum_scatter(
        lax.dot_general(
            mid_grad, activated, (((0,), (0,)), ((), ())), preferred_element_type=jnp.float32
        ).astype(jnp.bfloat16),
        "sp",
        scatter_dimension=0,
        tiled=True,
    ).astype(jnp.float32)
    return (grad_gate[None], grad_up[None], grad_down[None], grad_proj, conv_input_grad)


def dispatch_kernel(send_m, send_c, send_w, out_m, out_c, out_w, s_sem, r_sem, w_sem, l_sem):
    sp, tp = lax.axis_index("sp"), lax.axis_index("tp")
    planes, slots, width = send_m.shape
    plane, side = sp // TOP, sp % TOP
    row, core = tp // 2, tp % 2
    across = (TOP * plane + 1 - side, tp)
    along = (sp, 2 * (1 - row) + core)
    partner = (sp, 2 * row + 1 - core)

    barrier = pltpu.get_barrier_semaphore()
    targets = [across, along, partner]
    targets += [(TOP * ((plane + k) % planes) + side, tp) for k in range(1, planes)]
    for target in targets:
        pl.semaphore_signal(barrier, inc=1, device_id=target, device_id_type=MESH)
    pl.semaphore_wait(barrier, len(targets))

    sends = (send_m, send_c)
    outs = (out_m, out_c)

    def place(array, block, quarter):
        return outs[array].at[block, :, pl.ds(pl.multiple_of(quarter * width, width), width)]

    def remote(source, target_ref, kind, k, array, device):
        return pltpu.make_async_remote_copy(
            src_ref=source,
            dst_ref=target_ref,
            send_sem=s_sem.at[kind, k, array],
            recv_sem=r_sem.at[kind, k, array],
            device_id=device,
            device_id_type=MESH,
        )

    def weights(source, block, kind, k, device):
        return pltpu.make_async_remote_copy(
            src_ref=source,
            dst_ref=out_w.at[block],
            send_sem=w_sem.at[0, kind, k],
            recv_sem=w_sem.at[1, kind, k],
            device_id=device,
            device_id_type=MESH,
        )

    copies = []
    arrivals = {}
    own = TOP * plane + side
    for k in range(1, planes):
        to = (plane - k + planes) % planes
        device = (TOP * to + side, tp)
        for array in range(2):
            copy = remote(sends[array].at[to], place(array, own, tp), 0, k, array, device)
            copy.start()
            copies.append(copy)
            arrivals[0, k, array] = copy
        copy = weights(send_w.at[to], own, 0, k, device)
        copy.start()
        copies.append(copy)
        arrivals[0, k, 2] = copy

    local = []
    for array in range(2):
        local.append(pltpu.make_async_copy(sends[array].at[plane], place(array, own, tp), l_sem.at[array]))
    local.append(pltpu.make_async_copy(send_w.at[plane], out_w.at[own], l_sem.at[2]))
    for copy in local:
        copy.start()

    def forward(kind, k, array, block, quarter, device, source=None):
        ref = place(array, block, quarter)
        copy = remote(ref if source is None else source, ref, kind, k, array, device)
        copy.start()
        copies.append(copy)
        arrivals[kind, k, array] = copy

    other = 2 * (1 - row) + core
    for step in range(planes + 2):
        k = step
        if k < planes:
            block = TOP * ((plane + k) % planes) + side
            for array in range(2):
                if k > 0:
                    arrivals[0, k, array].wait_recv()
                source = sends[array].at[plane] if k == 0 else None
                forward(1, k, array, block, tp, across, source)
                forward(2, k, array, block, tp, along, source)
                forward(3, k, array, block, tp, partner, source)
            if k > 0:
                arrivals[0, k, 2].wait_recv()
            source = send_w.at[plane] if k == 0 else out_w.at[block]
            copy = weights(source, block, 1, k, across)
            copy.start()
            copies.append(copy)
            arrivals[1, k, 2] = copy
        k = step - 1
        if 0 <= k < planes:
            mine = TOP * ((plane + k) % planes) + side
            theirs = TOP * ((plane + k) % planes) + 1 - side
            arrivals[1, k, 0].wait_recv()
            forward(4, k, 0, theirs, tp, along)
            forward(5, k, 0, theirs, tp, partner)
            arrivals[2, k, 1].wait_recv()
            forward(4, k, 1, mine, other, across)
            forward(6, k, 1, mine, other, partner)
            arrivals[1, k, 1].wait_recv()
            forward(5, k, 1, theirs, tp, partner)
            arrivals[2, k, 0].wait_recv()
            forward(6, k, 0, mine, other, partner)
            arrivals[1, k, 2].wait_recv()
        k = step - 2
        if 0 <= k < planes:
            theirs = TOP * ((plane + k) % planes) + 1 - side
            for array in range(2):
                arrivals[4, k, array].wait_recv()
                forward(7, k, array, theirs, other, partner)
    for k in range(planes):
        for array in range(2):
            for kind in (3, 5, 6, 7):
                arrivals[kind, k, array].wait_recv()
    for copy in copies:
        copy.wait_send()
    for copy in local:
        copy.wait()


def dispatch(send_m, send_c, send_w):
    planes, slots, width = send_m.shape
    blocks = lax.axis_size("sp")
    vmem = pl.BlockSpec(memory_space=pltpu.VMEM)
    rows = jax.ShapeDtypeStruct((blocks, slots, width * lax.axis_size("tp")), send_m.dtype)
    return pl.pallas_call(
        dispatch_kernel,
        out_shape=(rows, rows, jax.ShapeDtypeStruct((blocks,) + send_w.shape[1:], send_w.dtype)),
        in_specs=[vmem] * 3,
        out_specs=(vmem, vmem, vmem),
        scratch_shapes=[
            pltpu.SemaphoreType.DMA((8, planes, 2)),
            pltpu.SemaphoreType.DMA((8, planes, 2)),
            pltpu.SemaphoreType.DMA((2, 2, planes)),
            pltpu.SemaphoreType.DMA((3,)),
        ],
        compiler_params=pltpu.CompilerParams(
            collective_id=0, has_side_effects=True, vmem_limit_bytes=32 * 1024 * 1024
        ),
        name="dispatch",
    )(send_m, send_c, send_w)


def dot(left, right, left_dim, right_dim):
    return lax.dot_general(
        left, right, (((left_dim,), (right_dim,)), ((), ())), preferred_element_type=jnp.float32
    )


def paired_body(
    mid_state,
    conv_pre,
    conv_taps,
    out_proj,
    route_expert,
    route_weight,
    gate_w,
    up_w,
    down_w,
    cotangent,
):
    experts = lax.axis_size("sp")
    tp_count = lax.axis_size("tp")
    token_count = mid_state.shape[0]
    slot_count = 17 * token_count * TOP // (16 * experts)
    slots = (slot_count + 7) // 8 * 8
    width = D // tp_count
    tp = lax.axis_index("tp")

    group = route_expert[:, 0] // TOP
    in_group = group[None, :] == jnp.arange(GROUPS, dtype=jnp.int32)[:, None]
    positions = jnp.arange(token_count, dtype=jnp.int32)
    earlier = (positions[:, None] < positions[None, :]).astype(jnp.bfloat16)
    ranks = dot(in_group.astype(jnp.bfloat16), earlier, 1, 0)
    rank = jnp.sum(jnp.where(in_group, ranks, 0.0), axis=0).astype(jnp.int32)
    slot = jnp.where(rank < slot_count, group * slots + rank, -1)
    taken = slot[None, :] == jnp.arange(GROUPS * slots, dtype=jnp.int32)[:, None]
    pick = taken.astype(jnp.bfloat16)
    own_state = lax.dynamic_slice_in_dim(mid_state, tp * width, width, 1)
    own_cot = lax.dynamic_slice_in_dim(cotangent, tp * width, width, 1)
    send_m = dot(pick, own_state, 1, 0).astype(jnp.bfloat16).reshape(GROUPS, slots, width)
    send_c = dot(pick, own_cot, 1, 0).astype(jnp.bfloat16).reshape(GROUPS, slots, width)
    swapped = (route_expert[:, 0] % TOP) != 0
    first = jnp.where(swapped, route_weight[:, 1], route_weight[:, 0])
    second = jnp.where(swapped, route_weight[:, 0], route_weight[:, 1])
    slot_weights = [
        jnp.sum(jnp.where(taken, each[None, :], 0.0), axis=1).reshape(GROUPS, 1, slots)
        for each in (first, second)
    ]
    send_w = jnp.pad(
        jnp.concatenate(slot_weights, axis=1), ((0, 0), (0, 8 - TOP), (0, -slots % 128))
    )
    got_m, got_c, got_w = dispatch(send_m, send_c, send_w)
    inputs = got_m.reshape(experts * slots, D)
    side = lax.axis_index("sp") % TOP
    weight = lax.dynamic_index_in_dim(got_w, side, 1, keepdims=False)[:, :slots]
    seeds = (
        (weight[:, :, None] * got_c.astype(jnp.float32))
        .astype(jnp.bfloat16)
        .reshape(experts * slots, D)
    )
    gate_mat = gate_w[0]
    up_mat = up_w[0]
    down_mat = down_w[0]
    gate_pre = dot(inputs, gate_mat, 1, 0)
    up_pre = dot(inputs, up_mat, 1, 0)
    gate_act = jax.nn.silu(gate_pre)
    hidden = (gate_act * up_pre).astype(jnp.bfloat16)
    hidden_grad = dot(seeds, down_mat, 1, 1)
    gate_grad = (hidden_grad * up_pre * silu_slope(gate_pre)).astype(jnp.bfloat16)
    up_grad = (hidden_grad * gate_act).astype(jnp.bfloat16)
    partial_value = (dot(gate_grad, gate_mat, 1, 1) + dot(up_grad, up_mat, 1, 1)).astype(
        jnp.bfloat16
    )
    summed = lax.psum_scatter(partial_value, "tp", scatter_dimension=1, tiled=True)
    returned = lax.all_to_all(
        summed.reshape(experts, slots, width), "sp", split_axis=0, concat_axis=0, tiled=True
    )
    pick_each = jnp.repeat(pick.reshape(GROUPS, 1, slots, token_count), TOP, axis=1)
    moe_grad = dot(
        pick_each.reshape(experts * slots, token_count),
        returned.reshape(experts * slots, width),
        0,
        0,
    )
    mid_part = (own_cot.astype(jnp.float32) + moe_grad).astype(jnp.bfloat16)
    mid_grad = lax.all_gather(mid_part, "tp", axis=1, tiled=True)
    grad_down = dot(hidden, seeds, 0, 0).astype(jnp.bfloat16)
    grad_gate = dot(inputs, gate_grad, 0, 0).astype(jnp.bfloat16)
    grad_up = dot(inputs, up_grad, 0, 0).astype(jnp.bfloat16)
    pre_float = conv_pre.astype(jnp.float32)
    activated = jax.nn.silu(pre_float).astype(jnp.bfloat16)
    mixed_grad = dot(mid_grad, out_proj, 1, 1)
    conv_grad = (mixed_grad * silu_slope(pre_float)).astype(jnp.bfloat16)
    next_head = passed_along(conv_grad[: KERNEL - 1], "sp", -1)
    extended = jnp.concatenate([conv_grad, next_head], axis=0).astype(jnp.float32)
    conv_input_grad = jnp.zeros(conv_grad.shape, jnp.float32)
    for lag_index in range(KERNEL):
        conv_input_grad = (
            conv_input_grad
            + conv_taps[lag_index].astype(jnp.float32)[None, :]
            * extended[lag_index : lag_index + token_count]
        )
    grad_proj = lax.psum_scatter(
        dot(mid_grad, activated, 0, 0).astype(jnp.bfloat16),
        "sp",
        scatter_dimension=0,
        tiled=True,
    ).astype(jnp.float32)
    return (grad_gate[None], grad_up[None], grad_down[None], grad_proj, conv_input_grad)


def solution(mesh):
    placed = (
        P("sp", None),
        P("sp", "tp"),
        P(None, "tp"),
        P("tp", None),
        P("sp", None),
        P("sp", None),
        P("sp", None, "tp"),
        P("sp", None, "tp"),
        P("sp", "tp", None),
        P("sp", None),
    )
    experts = mesh.shape["sp"]
    paired = experts == GROUPS * TOP and mesh.shape["tp"] == 4
    return jax.shard_map(
        paired_body if paired else body,
        mesh=mesh,
        in_specs=placed,
        out_specs=(
            P("sp", None, "tp"),
            P("sp", None, "tp"),
            P("sp", "tp", None),
            P("sp", "tp"),
            P("sp", "tp"),
        ),
        check_vma=False,
    )
```

```python
import jax
import jax.numpy as jnp
from jax import lax
from jax.experimental import pallas as pl
from jax.experimental.pallas import tpu as pltpu
from jax.sharding import PartitionSpec as P

D = 2048
KERNEL = 31
TOP = 2
GROUPS = 4
MESH = pl.DeviceIdType.MESH


def passed_along(value, axis, steps):
    count = lax.axis_size(axis)
    initial, last = (max(0, -steps), min(count, count - steps))
    return lax.ppermute(value, axis, [(source, source + steps) for source in range(initial, last)])


def silu_slope(value):
    sig = jax.nn.sigmoid(value)
    return sig * (1.0 + value * (1.0 - sig))


def body(
    mid_state,
    conv_pre,
    conv_taps,
    out_proj,
    route_expert,
    route_weight,
    gate_w,
    up_w,
    down_w,
    cotangent,
):
    groups = lax.axis_size("sp")
    token_count = mid_state.shape[0]
    slot_count = 17 * token_count * TOP // (16 * groups)
    flat_routes = route_expert.reshape(-1)
    one_hot_table = (flat_routes[:, None] == jnp.arange(groups, dtype=jnp.int32)[None, :]).astype(
        jnp.int32
    )
    slot_rank = jnp.sum(jnp.cumsum(one_hot_table, axis=0) * one_hot_table, axis=1) - 1
    kept_mask = slot_rank < slot_count
    slot_index = jnp.where(kept_mask, flat_routes * slot_count + slot_rank, groups * slot_count)
    token_ids = jnp.arange(token_count * TOP, dtype=jnp.int32) // TOP
    route_cot = (
        route_weight.reshape(-1)[:, None] * cotangent[token_ids].astype(jnp.float32)
    ).astype(jnp.bfloat16)
    send_inputs = (
        jnp.zeros((groups * slot_count, D), jnp.bfloat16)
        .at[slot_index]
        .set(mid_state[token_ids], mode="drop")
        .reshape(groups, slot_count, D)
    )
    send_seeds = (
        jnp.zeros((groups * slot_count, D), jnp.bfloat16)
        .at[slot_index]
        .set(route_cot, mode="drop")
        .reshape(groups, slot_count, D)
    )
    got_inputs, got_seeds = (
        lax.all_to_all(send_inputs, "sp", split_axis=0, concat_axis=0, tiled=True),
        lax.all_to_all(send_seeds, "sp", split_axis=0, concat_axis=0, tiled=True),
    )
    inputs = got_inputs.reshape(groups * slot_count, D)
    seeds = got_seeds.reshape(groups * slot_count, D)
    gate_mat = gate_w[0]
    up_mat = up_w[0]
    down_mat = down_w[0]
    gate_pre = jnp.dot(inputs, gate_mat, preferred_element_type=jnp.float32)
    up_pre = jnp.dot(inputs, up_mat, preferred_element_type=jnp.float32)
    gate_act = jax.nn.silu(gate_pre)
    hidden = (gate_act * up_pre).astype(jnp.bfloat16)
    hidden_grad = lax.dot_general(
        seeds, down_mat, (((1,), (1,)), ((), ())), preferred_element_type=jnp.float32
    )
    gate_grad = (hidden_grad * up_pre * silu_slope(gate_pre)).astype(jnp.bfloat16)
    up_grad = (hidden_grad * gate_act).astype(jnp.bfloat16)
    grad_down = lax.dot_general(
        hidden, seeds, (((0,), (0,)), ((), ())), preferred_element_type=jnp.float32
    ).astype(jnp.bfloat16)
    grad_gate = lax.dot_general(
        inputs, gate_grad, (((0,), (0,)), ((), ())), preferred_element_type=jnp.float32
    ).astype(jnp.bfloat16)
    grad_up = lax.dot_general(
        inputs, up_grad, (((0,), (0,)), ((), ())), preferred_element_type=jnp.float32
    ).astype(jnp.bfloat16)
    weight_results = (grad_gate, grad_up, grad_down)
    partial_value = lax.dot_general(
        gate_grad, gate_mat, (((1,), (1,)), ((), ())), preferred_element_type=jnp.float32
    )
    partial_value = partial_value + lax.dot_general(
        up_grad, up_mat, (((1,), (1,)), ((), ())), preferred_element_type=jnp.float32
    )
    partial_value = partial_value.astype(jnp.bfloat16).astype(jnp.float32)
    safe_index = jnp.minimum(slot_index, groups * slot_count - 1)
    slice_width = D // lax.axis_size("tp")
    summed = lax.psum_scatter(
        partial_value.astype(jnp.bfloat16), "tp", scatter_dimension=1, tiled=True
    )
    returned = lax.all_to_all(
        summed.reshape(groups, slot_count, slice_width),
        "sp",
        split_axis=0,
        concat_axis=0,
        tiled=True,
    ).reshape(groups * slot_count, slice_width)
    picked = jnp.where(
        kept_mask[:, None], returned[safe_index].astype(jnp.float32), jnp.float32(0.0)
    )
    moe_grad = jnp.sum(picked.reshape(token_count, TOP, slice_width), axis=1)
    own_cot = lax.dynamic_slice_in_dim(
        cotangent, lax.axis_index("tp") * slice_width, slice_width, 1
    )
    mid_part = (own_cot.astype(jnp.float32) + moe_grad).astype(jnp.bfloat16)
    mid_grad = lax.all_gather(mid_part, "tp", axis=1, tiled=True)
    grad_gate, grad_up, grad_down = weight_results
    pre_float = conv_pre.astype(jnp.float32)
    activated = jax.nn.silu(pre_float).astype(jnp.bfloat16)
    mixed_grad = lax.dot_general(
        mid_grad, out_proj, (((1,), (1,)), ((), ())), preferred_element_type=jnp.float32
    )
    conv_grad = (mixed_grad * silu_slope(pre_float)).astype(jnp.bfloat16)
    next_head = passed_along(conv_grad[: KERNEL - 1], "sp", -1)
    extended = jnp.concatenate([conv_grad, next_head], axis=0).astype(jnp.float32)
    conv_input_grad = jnp.zeros(conv_grad.shape, jnp.float32)
    for lag_index in range(KERNEL):
        conv_input_grad = (
            conv_input_grad
            + conv_taps[lag_index].astype(jnp.float32)[None, :]
            * extended[lag_index : lag_index + token_count]
        )
    grad_proj = lax.psum_scatter(
        lax.dot_general(
            mid_grad, activated, (((0,), (0,)), ((), ())), preferred_element_type=jnp.float32
        ).astype(jnp.bfloat16),
        "sp",
        scatter_dimension=0,
        tiled=True,
    ).astype(jnp.float32)
    return (grad_gate[None], grad_up[None], grad_down[None], grad_proj, conv_input_grad)


def dispatch_kernel(send_m, send_c, send_w, out_m, out_c, out_w, s_sem, r_sem, w_sem, l_sem):
    sp, tp = lax.axis_index("sp"), lax.axis_index("tp")
    planes, slots, width = send_m.shape
    plane, side = sp // TOP, sp % TOP
    row, core = tp // 2, tp % 2
    across = (TOP * plane + 1 - side, tp)
    along = (sp, 2 * (1 - row) + core)
    partner = (sp, 2 * row + 1 - core)

    barrier = pltpu.get_barrier_semaphore()
    targets = [across, along, partner]
    targets += [(TOP * ((plane + k) % planes) + side, tp) for k in range(1, planes)]
    for target in targets:
        pl.semaphore_signal(barrier, inc=1, device_id=target, device_id_type=MESH)
    pl.semaphore_wait(barrier, len(targets))

    sends = (send_m, send_c)
    outs = (out_m, out_c)

    def place(array, block, quarter):
        return outs[array].at[block, :, pl.ds(pl.multiple_of(quarter * width, width), width)]

    def remote(source, target_ref, kind, k, array, device):
        return pltpu.make_async_remote_copy(
            src_ref=source,
            dst_ref=target_ref,
            send_sem=s_sem.at[kind, k, array],
            recv_sem=r_sem.at[kind, k, array],
            device_id=device,
            device_id_type=MESH,
        )

    def weights(source, block, kind, k, device):
        return pltpu.make_async_remote_copy(
            src_ref=source,
            dst_ref=out_w.at[block],
            send_sem=w_sem.at[0, kind, k],
            recv_sem=w_sem.at[1, kind, k],
            device_id=device,
            device_id_type=MESH,
        )

    copies = []
    arrivals = {}
    own = TOP * plane + side
    for k in range(1, planes):
        to = (plane - k + planes) % planes
        device = (TOP * to + side, tp)
        for array in range(2):
            copy = remote(sends[array].at[to], place(array, own, tp), 0, k, array, device)
            copy.start()
            copies.append(copy)
            arrivals[0, k, array] = copy
        copy = weights(send_w.at[to], own, 0, k, device)
        copy.start()
        copies.append(copy)
        arrivals[0, k, 2] = copy

    local = []
    for array in range(2):
        local.append(pltpu.make_async_copy(sends[array].at[plane], place(array, own, tp), l_sem.at[array]))
    local.append(pltpu.make_async_copy(send_w.at[plane], out_w.at[own], l_sem.at[2]))
    for copy in local:
        copy.start()

    def forward(kind, k, array, block, quarter, device, source=None):
        ref = place(array, block, quarter)
        copy = remote(ref if source is None else source, ref, kind, k, array, device)
        copy.start()
        copies.append(copy)
        arrivals[kind, k, array] = copy

    other = 2 * (1 - row) + core
    for step in range(planes + 2):
        k = step
        if k < planes:
            block = TOP * ((plane + k) % planes) + side
            for array in range(2):
                if k > 0:
                    arrivals[0, k, array].wait_recv()
                source = sends[array].at[plane] if k == 0 else None
                forward(1, k, array, block, tp, across, source)
                forward(2, k, array, block, tp, along, source)
                forward(3, k, array, block, tp, partner, source)
            if k > 0:
                arrivals[0, k, 2].wait_recv()
            source = send_w.at[plane] if k == 0 else out_w.at[block]
            copy = weights(source, block, 1, k, across)
            copy.start()
            copies.append(copy)
            arrivals[1, k, 2] = copy
        k = step - 1
        if 0 <= k < planes:
            mine = TOP * ((plane + k) % planes) + side
            theirs = TOP * ((plane + k) % planes) + 1 - side
            arrivals[1, k, 0].wait_recv()
            forward(4, k, 0, theirs, tp, along)
            forward(5, k, 0, theirs, tp, partner)
            arrivals[2, k, 1].wait_recv()
            forward(4, k, 1, mine, other, across)
            forward(6, k, 1, mine, other, partner)
            arrivals[1, k, 1].wait_recv()
            forward(5, k, 1, theirs, tp, partner)
            arrivals[2, k, 0].wait_recv()
            forward(6, k, 0, mine, other, partner)
            arrivals[1, k, 2].wait_recv()
        k = step - 2
        if 0 <= k < planes:
            theirs = TOP * ((plane + k) % planes) + 1 - side
            for array in range(2):
                arrivals[4, k, array].wait_recv()
                forward(7, k, array, theirs, other, partner)
    for k in range(planes):
        for array in range(2):
            for kind in (3, 5, 6, 7):
                arrivals[kind, k, array].wait_recv()
    for copy in copies:
        copy.wait_send()
    for copy in local:
        copy.wait()


def dispatch(send_m, send_c, send_w):
    planes, slots, width = send_m.shape
    blocks = lax.axis_size("sp")
    vmem = pl.BlockSpec(memory_space=pltpu.VMEM)
    rows = jax.ShapeDtypeStruct((blocks, slots, width * lax.axis_size("tp")), send_m.dtype)
    return pl.pallas_call(
        dispatch_kernel,
        out_shape=(rows, rows, jax.ShapeDtypeStruct((blocks,) + send_w.shape[1:], send_w.dtype)),
        in_specs=[vmem] * 3,
        out_specs=(vmem, vmem, vmem),
        scratch_shapes=[
            pltpu.SemaphoreType.DMA((8, planes, 2)),
            pltpu.SemaphoreType.DMA((8, planes, 2)),
            pltpu.SemaphoreType.DMA((2, 2, planes)),
            pltpu.SemaphoreType.DMA((3,)),
        ],
        compiler_params=pltpu.CompilerParams(
            collective_id=0, has_side_effects=True, vmem_limit_bytes=32 * 1024 * 1024
        ),
        name="dispatch",
    )(send_m, send_c, send_w)


def neighbours():
    sp, tp = lax.axis_index("sp"), lax.axis_index("tp")
    plane, side = sp // TOP, sp % TOP
    row, core = tp // 2, tp % 2
    across = (TOP * plane + 1 - side, tp)
    along = (sp, 2 * (1 - row) + core)
    partner = (sp, 2 * row + 1 - core)
    return plane, side, row, core, across, along, partner


def greet(targets):
    barrier = pltpu.get_barrier_semaphore()
    for target in targets:
        pl.semaphore_signal(barrier, inc=1, device_id=target, device_id_type=MESH)
    pl.semaphore_wait(barrier, len(targets))


def wide(value):
    return value.astype(jnp.float32)


def give_back_kernel(
    part, pick, cot, out, pair_in, pair_sum, in_y, in_x, sum_y, sum_x, last_x, last_y, total, back,
    s_sem, r_sem, g_sem
):
    planes, _, width = back.shape
    half = width // 2
    plane, side, row, core, across, along, partner = neighbours()
    tp = 2 * row + core
    tp_other = 2 * (1 - row) + core
    greet(
        [across, along, partner]
        + [(TOP * ((plane + k) % planes) + side, tp) for k in range(1, planes)]
    )
    copies = []
    arrivals = {}

    def remote(source, target_ref, sems, kind, k, device):
        copy = pltpu.make_async_remote_copy(
            src_ref=source,
            dst_ref=target_ref,
            send_sem=sems[0],
            recv_sem=sems[1],
            device_id=device,
            device_id_type=MESH,
        )
        copy.start()
        copies.append(copy)
        arrivals[kind, k] = copy

    def sems(kind, k):
        return s_sem.at[kind, k], r_sem.at[kind, k]

    def columns(quarter):
        return pl.ds(pl.multiple_of(quarter * width, width), width)

    rows_of = [TOP * ((plane + k + 1) % planes) for k in range(planes)]
    for k in range(planes):
        for j in range(2):
            quarter = 2 * (row if j == 0 else 1 - row) + 1 - core
            remote(
                part.at[pl.ds(rows_of[k], TOP), :, columns(quarter)],
                pair_in.at[k, j], sems(j, k), j, k, partner,
            )
    low, high = pl.ds(0, half), pl.ds(half, half)
    for step in range(planes + 2):
        k = step
        if k < planes:
            for j, quarter in ((0, tp), (1, tp_other)):
                arrivals[j, k].wait_recv()
                pair_sum[k, j] = (
                    wide(part[pl.ds(rows_of[k], TOP), :, columns(quarter)]) + wide(pair_in[k, j])
                ).astype(out.dtype)
            remote(pair_sum.at[k, 1, :, :, low], in_y.at[k], sems(2, k), 2, k, along)
            remote(pair_sum.at[k, :, 1 - side, :, high], in_x.at[k], sems(3, k), 3, k, across)
        k = step - 1
        if 0 <= k < planes:
            arrivals[2, k].wait_recv()
            sum_y[k] = (wide(pair_sum[k, 0, :, :, low]) + wide(in_y[k])).astype(out.dtype)
            remote(sum_y.at[k, 1 - side], last_x.at[k], sems(4, k), 4, k, across)
            arrivals[3, k].wait_recv()
            sum_x[k] = (wide(pair_sum[k, :, side, :, high]) + wide(in_x[k])).astype(out.dtype)
            remote(sum_x.at[k, 1], last_y.at[k], sems(5, k), 5, k, along)
        k = step - 2
        if 0 <= k < planes:
            arrivals[4, k].wait_recv()
            arrivals[5, k].wait_recv()
            total[k, :, low] = (wide(sum_y[k, side]) + wide(last_x[k])).astype(out.dtype)
            total[k, :, high] = (wide(sum_x[k, 0]) + wide(last_y[k])).astype(out.dtype)
            if k < planes - 1:
                to = (TOP * ((plane + k + 1) % planes) + side, tp)
                remote(total.at[k], back.at[plane], sems(6, k), 6, k, to)
    moe = jnp.dot(pick[plane], total[planes - 1], preferred_element_type=jnp.float32)
    for k in range(planes - 1):
        arrivals[6, k].wait_recv()
        source = (plane + planes - k - 1) % planes
        moe += jnp.dot(pick[source], back[source], preferred_element_type=jnp.float32)
    out[:, columns(tp)] = (wide(cot[...]) + moe).astype(out.dtype)
    mine = out.at[:, columns(tp)]
    remote(mine, mine, (g_sem.at[0, 0], g_sem.at[1, 0]), 7, 0, along)
    remote(mine, mine, (g_sem.at[0, 1], g_sem.at[1, 1]), 7, 1, partner)
    arrivals[7, 0].wait_recv()
    theirs = out.at[:, columns(tp_other)]
    remote(theirs, theirs, (g_sem.at[0, 2], g_sem.at[1, 2]), 7, 2, partner)
    arrivals[7, 1].wait_recv()
    arrivals[7, 2].wait_recv()
    for copy in copies:
        copy.wait_send()


def give_back(part, pick, cot):
    planes, token_count, slots = pick.shape
    width = cot.shape[1]
    half = width // 2
    vmem = pl.BlockSpec(memory_space=pltpu.VMEM)
    dtype = part.dtype
    return pl.pallas_call(
        give_back_kernel,
        out_shape=jax.ShapeDtypeStruct((token_count, part.shape[2]), dtype),
        in_specs=[vmem] * 3,
        out_specs=vmem,
        scratch_shapes=[
            pltpu.VMEM((planes, 2, TOP, slots, width), dtype),
            pltpu.VMEM((planes, 2, TOP, slots, width), dtype),
            pltpu.VMEM((planes, TOP, slots, half), dtype),
            pltpu.VMEM((planes, 2, slots, half), dtype),
            pltpu.VMEM((planes, TOP, slots, half), dtype),
            pltpu.VMEM((planes, 2, slots, half), dtype),
            pltpu.VMEM((planes, slots, half), dtype),
            pltpu.VMEM((planes, slots, half), dtype),
            pltpu.VMEM((planes, slots, width), dtype),
            pltpu.VMEM((planes, slots, width), dtype),
            pltpu.SemaphoreType.DMA((7, planes)),
            pltpu.SemaphoreType.DMA((7, planes)),
            pltpu.SemaphoreType.DMA((2, 3)),
        ],
        compiler_params=pltpu.CompilerParams(
            collective_id=1, has_side_effects=True, vmem_limit_bytes=40 * 1024 * 1024
        ),
        name="give_back",
    )(part, pick, cot)


def reduce_kernel(prod, out, in_x, side_sum, in_z, s_sem, r_sem):
    planes = in_x.shape[0]
    plane, side, row, core, across, _, _ = neighbours()
    tp = 2 * row + core
    to = [(TOP * ((plane + k + 1) % planes) + side, tp) for k in range(planes - 1)]
    greet([across] + to)

    def remote(source, target_ref, kind, k, device):
        copy = pltpu.make_async_remote_copy(
            src_ref=source,
            dst_ref=target_ref,
            send_sem=s_sem.at[kind, k],
            recv_sem=r_sem.at[kind, k],
            device_id=device,
            device_id_type=MESH,
        )
        copy.start()
        return copy

    rows_of = [TOP * ((plane + k + 1) % planes) for k in range(planes)]
    crossing = [
        remote(prod.at[rows_of[k] + 1 - side], in_x.at[k], 0, k, across) for k in range(planes)
    ]
    climbing = []
    for k in range(planes):
        crossing[k].wait_recv()
        both = wide(prod[rows_of[k] + side]) + wide(in_x[k])
        if k < planes - 1:
            side_sum[k] = both.astype(prod.dtype)
            climbing.append(remote(side_sum.at[k], in_z.at[k], 1, k, to[k]))
    for k in range(planes - 1):
        climbing[k].wait_recv()
        both += wide(in_z[k])
    out[...] = both
    for copy in crossing + climbing:
        copy.wait_send()


def reduce_rows(prod):
    blocks, rows, width = prod.shape
    planes = blocks // TOP
    vmem = pl.BlockSpec(memory_space=pltpu.VMEM)
    return pl.pallas_call(
        reduce_kernel,
        out_shape=jax.ShapeDtypeStruct((rows, width), jnp.float32),
        in_specs=[vmem],
        out_specs=vmem,
        scratch_shapes=[
            pltpu.VMEM((planes, rows, width), prod.dtype),
            pltpu.VMEM((planes - 1, rows, width), prod.dtype),
            pltpu.VMEM((planes - 1, rows, width), prod.dtype),
            pltpu.SemaphoreType.DMA((2, planes)),
            pltpu.SemaphoreType.DMA((2, planes)),
        ],
        compiler_params=pltpu.CompilerParams(
            collective_id=2, has_side_effects=True, vmem_limit_bytes=32 * 1024 * 1024
        ),
        name="reduce_rows",
    )(prod)


def dot(left, right, left_dim, right_dim):
    return lax.dot_general(
        left, right, (((left_dim,), (right_dim,)), ((), ())), preferred_element_type=jnp.float32
    )


def paired_body(
    mid_state,
    conv_pre,
    conv_taps,
    out_proj,
    route_expert,
    route_weight,
    gate_w,
    up_w,
    down_w,
    cotangent,
):
    experts = lax.axis_size("sp")
    tp_count = lax.axis_size("tp")
    token_count = mid_state.shape[0]
    slot_count = 17 * token_count * TOP // (16 * experts)
    slots = (slot_count + 7) // 8 * 8
    width = D // tp_count
    tp = lax.axis_index("tp")

    group = route_expert[:, 0] // TOP
    in_group = group[None, :] == jnp.arange(GROUPS, dtype=jnp.int32)[:, None]
    positions = jnp.arange(token_count, dtype=jnp.int32)
    earlier = (positions[:, None] < positions[None, :]).astype(jnp.bfloat16)
    ranks = dot(in_group.astype(jnp.bfloat16), earlier, 1, 0)
    rank = jnp.sum(jnp.where(in_group, ranks, 0.0), axis=0).astype(jnp.int32)
    slot = jnp.where(rank < slot_count, group * slots + rank, -1)
    taken = slot[None, :] == jnp.arange(GROUPS * slots, dtype=jnp.int32)[:, None]
    pick = taken.astype(jnp.bfloat16)
    own_state = lax.dynamic_slice_in_dim(mid_state, tp * width, width, 1)
    own_cot = lax.dynamic_slice_in_dim(cotangent, tp * width, width, 1)
    send_m = dot(pick, own_state, 1, 0).astype(jnp.bfloat16).reshape(GROUPS, slots, width)
    send_c = dot(pick, own_cot, 1, 0).astype(jnp.bfloat16).reshape(GROUPS, slots, width)
    swapped = (route_expert[:, 0] % TOP) != 0
    first = jnp.where(swapped, route_weight[:, 1], route_weight[:, 0])
    second = jnp.where(swapped, route_weight[:, 0], route_weight[:, 1])
    slot_weights = [
        jnp.sum(jnp.where(taken, each[None, :], 0.0), axis=1).reshape(GROUPS, 1, slots)
        for each in (first, second)
    ]
    send_w = jnp.pad(
        jnp.concatenate(slot_weights, axis=1), ((0, 0), (0, 8 - TOP), (0, -slots % 128))
    )
    got_m, got_c, got_w = dispatch(send_m, send_c, send_w)
    inputs = got_m.reshape(experts * slots, D)
    side = lax.axis_index("sp") % TOP
    weight = lax.dynamic_index_in_dim(got_w, side, 1, keepdims=False)[:, :slots]
    seeds = (
        (weight[:, :, None] * got_c.astype(jnp.float32))
        .astype(jnp.bfloat16)
        .reshape(experts * slots, D)
    )
    gate_mat = gate_w[0]
    up_mat = up_w[0]
    down_mat = down_w[0]
    gate_pre = dot(inputs, gate_mat, 1, 0)
    up_pre = dot(inputs, up_mat, 1, 0)
    gate_act = jax.nn.silu(gate_pre)
    hidden = (gate_act * up_pre).astype(jnp.bfloat16)
    hidden_grad = dot(seeds, down_mat, 1, 1)
    gate_grad = (hidden_grad * up_pre * silu_slope(gate_pre)).astype(jnp.bfloat16)
    up_grad = (hidden_grad * gate_act).astype(jnp.bfloat16)
    partial_value = (dot(gate_grad, gate_mat, 1, 1) + dot(up_grad, up_mat, 1, 1)).astype(
        jnp.bfloat16
    )
    own_slot = slot[None, :, None] == (
        slots * jnp.arange(GROUPS, dtype=jnp.int32)[:, None, None]
        + jnp.arange(slots, dtype=jnp.int32)[None, None, :]
    )
    mid_grad = give_back(
        partial_value.reshape(experts, slots, D), own_slot.astype(jnp.bfloat16), own_cot
    )
    grad_down = dot(hidden, seeds, 0, 0).astype(jnp.bfloat16)
    grad_gate = dot(inputs, gate_grad, 0, 0).astype(jnp.bfloat16)
    grad_up = dot(inputs, up_grad, 0, 0).astype(jnp.bfloat16)
    pre_float = conv_pre.astype(jnp.float32)
    activated = jax.nn.silu(pre_float).astype(jnp.bfloat16)
    mixed_grad = dot(mid_grad, out_proj, 1, 1)
    conv_grad = (mixed_grad * silu_slope(pre_float)).astype(jnp.bfloat16)
    next_head = passed_along(conv_grad[: KERNEL - 1], "sp", -1)
    extended = jnp.concatenate([conv_grad, next_head], axis=0).astype(jnp.float32)
    conv_input_grad = jnp.zeros(conv_grad.shape, jnp.float32)
    for lag_index in range(KERNEL):
        conv_input_grad = (
            conv_input_grad
            + conv_taps[lag_index].astype(jnp.float32)[None, :]
            * extended[lag_index : lag_index + token_count]
        )
    grad_proj = reduce_rows(
        dot(mid_grad, activated, 0, 0).astype(jnp.bfloat16).reshape(experts, D // experts, -1)
    )
    return (grad_gate[None], grad_up[None], grad_down[None], grad_proj, conv_input_grad)


def solution(mesh):
    placed = (
        P("sp", None),
        P("sp", "tp"),
        P(None, "tp"),
        P("tp", None),
        P("sp", None),
        P("sp", None),
        P("sp", None, "tp"),
        P("sp", None, "tp"),
        P("sp", "tp", None),
        P("sp", None),
    )
    experts = mesh.shape["sp"]
    paired = experts == GROUPS * TOP and mesh.shape["tp"] == 4
    return jax.shard_map(
        paired_body if paired else body,
        mesh=mesh,
        in_specs=placed,
        out_specs=(
            P("sp", None, "tp"),
            P("sp", None, "tp"),
            P("sp", "tp", None),
            P("sp", "tp"),
            P("sp", "tp"),
        ),
        check_vma=False,
    )
```

```python
import jax
import jax.numpy as jnp
from jax import lax
from jax.experimental import pallas as pl
from jax.experimental.pallas import tpu as pltpu
from jax.sharding import PartitionSpec as P

D = 2048
KERNEL = 31
TOP = 2
GROUPS = 4
MESH = pl.DeviceIdType.MESH


def passed_along(value, axis, steps):
    count = lax.axis_size(axis)
    initial, last = (max(0, -steps), min(count, count - steps))
    return lax.ppermute(value, axis, [(source, source + steps) for source in range(initial, last)])


def silu_slope(value):
    sig = jax.nn.sigmoid(value)
    return sig * (1.0 + value * (1.0 - sig))


def body(
    mid_state,
    conv_pre,
    conv_taps,
    out_proj,
    route_expert,
    route_weight,
    gate_w,
    up_w,
    down_w,
    cotangent,
):
    groups = lax.axis_size("sp")
    token_count = mid_state.shape[0]
    slot_count = 17 * token_count * TOP // (16 * groups)
    flat_routes = route_expert.reshape(-1)
    one_hot_table = (flat_routes[:, None] == jnp.arange(groups, dtype=jnp.int32)[None, :]).astype(
        jnp.int32
    )
    slot_rank = jnp.sum(jnp.cumsum(one_hot_table, axis=0) * one_hot_table, axis=1) - 1
    kept_mask = slot_rank < slot_count
    slot_index = jnp.where(kept_mask, flat_routes * slot_count + slot_rank, groups * slot_count)
    token_ids = jnp.arange(token_count * TOP, dtype=jnp.int32) // TOP
    route_cot = (
        route_weight.reshape(-1)[:, None] * cotangent[token_ids].astype(jnp.float32)
    ).astype(jnp.bfloat16)
    send_inputs = (
        jnp.zeros((groups * slot_count, D), jnp.bfloat16)
        .at[slot_index]
        .set(mid_state[token_ids], mode="drop")
        .reshape(groups, slot_count, D)
    )
    send_seeds = (
        jnp.zeros((groups * slot_count, D), jnp.bfloat16)
        .at[slot_index]
        .set(route_cot, mode="drop")
        .reshape(groups, slot_count, D)
    )
    got_inputs, got_seeds = (
        lax.all_to_all(send_inputs, "sp", split_axis=0, concat_axis=0, tiled=True),
        lax.all_to_all(send_seeds, "sp", split_axis=0, concat_axis=0, tiled=True),
    )
    inputs = got_inputs.reshape(groups * slot_count, D)
    seeds = got_seeds.reshape(groups * slot_count, D)
    gate_mat = gate_w[0]
    up_mat = up_w[0]
    down_mat = down_w[0]
    gate_pre = jnp.dot(inputs, gate_mat, preferred_element_type=jnp.float32)
    up_pre = jnp.dot(inputs, up_mat, preferred_element_type=jnp.float32)
    gate_act = jax.nn.silu(gate_pre)
    hidden = (gate_act * up_pre).astype(jnp.bfloat16)
    hidden_grad = lax.dot_general(
        seeds, down_mat, (((1,), (1,)), ((), ())), preferred_element_type=jnp.float32
    )
    gate_grad = (hidden_grad * up_pre * silu_slope(gate_pre)).astype(jnp.bfloat16)
    up_grad = (hidden_grad * gate_act).astype(jnp.bfloat16)
    grad_down = lax.dot_general(
        hidden, seeds, (((0,), (0,)), ((), ())), preferred_element_type=jnp.float32
    ).astype(jnp.bfloat16)
    grad_gate = lax.dot_general(
        inputs, gate_grad, (((0,), (0,)), ((), ())), preferred_element_type=jnp.float32
    ).astype(jnp.bfloat16)
    grad_up = lax.dot_general(
        inputs, up_grad, (((0,), (0,)), ((), ())), preferred_element_type=jnp.float32
    ).astype(jnp.bfloat16)
    weight_results = (grad_gate, grad_up, grad_down)
    partial_value = lax.dot_general(
        gate_grad, gate_mat, (((1,), (1,)), ((), ())), preferred_element_type=jnp.float32
    )
    partial_value = partial_value + lax.dot_general(
        up_grad, up_mat, (((1,), (1,)), ((), ())), preferred_element_type=jnp.float32
    )
    partial_value = partial_value.astype(jnp.bfloat16).astype(jnp.float32)
    safe_index = jnp.minimum(slot_index, groups * slot_count - 1)
    slice_width = D // lax.axis_size("tp")
    summed = lax.psum_scatter(
        partial_value.astype(jnp.bfloat16), "tp", scatter_dimension=1, tiled=True
    )
    returned = lax.all_to_all(
        summed.reshape(groups, slot_count, slice_width),
        "sp",
        split_axis=0,
        concat_axis=0,
        tiled=True,
    ).reshape(groups * slot_count, slice_width)
    picked = jnp.where(
        kept_mask[:, None], returned[safe_index].astype(jnp.float32), jnp.float32(0.0)
    )
    moe_grad = jnp.sum(picked.reshape(token_count, TOP, slice_width), axis=1)
    own_cot = lax.dynamic_slice_in_dim(
        cotangent, lax.axis_index("tp") * slice_width, slice_width, 1
    )
    mid_part = (own_cot.astype(jnp.float32) + moe_grad).astype(jnp.bfloat16)
    mid_grad = lax.all_gather(mid_part, "tp", axis=1, tiled=True)
    grad_gate, grad_up, grad_down = weight_results
    pre_float = conv_pre.astype(jnp.float32)
    activated = jax.nn.silu(pre_float).astype(jnp.bfloat16)
    mixed_grad = lax.dot_general(
        mid_grad, out_proj, (((1,), (1,)), ((), ())), preferred_element_type=jnp.float32
    )
    conv_grad = (mixed_grad * silu_slope(pre_float)).astype(jnp.bfloat16)
    next_head = passed_along(conv_grad[: KERNEL - 1], "sp", -1)
    extended = jnp.concatenate([conv_grad, next_head], axis=0).astype(jnp.float32)
    conv_input_grad = jnp.zeros(conv_grad.shape, jnp.float32)
    for lag_index in range(KERNEL):
        conv_input_grad = (
            conv_input_grad
            + conv_taps[lag_index].astype(jnp.float32)[None, :]
            * extended[lag_index : lag_index + token_count]
        )
    grad_proj = lax.psum_scatter(
        lax.dot_general(
            mid_grad, activated, (((0,), (0,)), ((), ())), preferred_element_type=jnp.float32
        ).astype(jnp.bfloat16),
        "sp",
        scatter_dimension=0,
        tiled=True,
    ).astype(jnp.float32)
    return (grad_gate[None], grad_up[None], grad_down[None], grad_proj, conv_input_grad)


def neighbours():
    sp, tp = lax.axis_index("sp"), lax.axis_index("tp")
    plane, side = sp // TOP, sp % TOP
    row, core = tp // 2, tp % 2
    across = (TOP * plane + 1 - side, tp)
    along = (sp, 2 * (1 - row) + core)
    partner = (sp, 2 * row + 1 - core)
    return plane, side, row, core, across, along, partner


def greet(targets):
    barrier = pltpu.get_barrier_semaphore()
    for target in targets:
        pl.semaphore_signal(barrier, inc=1, device_id=target, device_id_type=MESH)
    pl.semaphore_wait(barrier, len(targets))


def wide(value):
    return value.astype(jnp.float32)


def exchange_kernel(
    send_m, send_c, send_w, pick, cot, gate_hbm, up_hbm, down_hbm,
    out, out_m, out_seed, out_hidden, out_gate, out_up,
    out_c, out_w, gate_w, up_w, down_w, part,
    pair_in, pair_sum, in_y, in_x, sum_y, sum_x, last_x, last_y, total, back,
    s_sem, r_sem, w_sem, l_sem, s2_sem, r2_sem, g_sem
):
    planes, slots, width = send_m.shape
    half = width // 2
    plane, side, row, core, across, along, partner = neighbours()
    own = TOP * plane + side
    tp = 2 * row + core
    other = 2 * (1 - row) + core
    sends = (send_m, send_c)
    outs = (out_m, out_c)

    loads = [
        pltpu.make_async_copy(source, target, l_sem.at[3 + i])
        for i, (source, target) in enumerate(
            ((gate_hbm, gate_w), (up_hbm, up_w), (down_hbm, down_w))
        )
    ]
    for load in loads:
        load.start()
    greet(
        [across, along, partner]
        + [(TOP * ((plane + k) % planes) + side, tp) for k in range(1, planes)]
    )
    copies = []
    arrivals = {}

    def columns(quarter):
        return pl.ds(pl.multiple_of(quarter * width, width), width)

    def place(array, block, quarter):
        return outs[array].at[block, :, columns(quarter)]

    def remote(source, target_ref, send_sem, recv_sem, key, device):
        copy = pltpu.make_async_remote_copy(
            src_ref=source,
            dst_ref=target_ref,
            send_sem=send_sem,
            recv_sem=recv_sem,
            device_id=device,
            device_id_type=MESH,
        )
        copy.start()
        copies.append(copy)
        arrivals[key] = copy

    def move(source, target_ref, kind, k, array, device):
        remote(
            source, target_ref, s_sem.at[kind, k, array], r_sem.at[kind, k, array],
            (kind, k, array), device,
        )

    def weights(source, block, kind, k, device):
        remote(
            source, out_w.at[block], w_sem.at[0, kind, k], w_sem.at[1, kind, k],
            (kind, k, 2), device,
        )

    def give(source, target_ref, kind, k, device):
        remote(
            source, target_ref, s2_sem.at[kind, k], r2_sem.at[kind, k], ("give", kind, k), device
        )

    def got(kind, k):
        arrivals["give", kind, k].wait_recv()

    for k in range(1, planes):
        to = (plane - k + planes) % planes
        device = (TOP * to + side, tp)
        for array in range(2):
            move(sends[array].at[to], place(array, own, tp), 0, k, array, device)
        weights(send_w.at[to], own, 0, k, device)
    local = [
        pltpu.make_async_copy(sends[array].at[plane], place(array, own, tp), l_sem.at[array])
        for array in range(2)
    ]
    local.append(pltpu.make_async_copy(send_w.at[plane], out_w.at[own], l_sem.at[2]))
    for copy in local:
        copy.start()

    def forward(kind, k, array, block, quarter, device, source=None):
        ref = place(array, block, quarter)
        move(ref if source is None else source, ref, kind, k, array, device)

    low, high = pl.ds(0, half), pl.ds(half, half)
    for step in range(planes + 6):
        k = step
        if k < planes:
            block = TOP * ((plane + k) % planes) + side
            for array in range(2):
                if k > 0:
                    arrivals[0, k, array].wait_recv()
                source = sends[array].at[plane] if k == 0 else None
                forward(1, k, array, block, tp, across, source)
                forward(2, k, array, block, tp, along, source)
                forward(3, k, array, block, tp, partner, source)
            if k > 0:
                arrivals[0, k, 2].wait_recv()
            weights(send_w.at[plane] if k == 0 else out_w.at[block], block, 1, k, across)
        k = step - 1
        if 0 <= k < planes:
            mine = TOP * ((plane + k) % planes) + side
            theirs = TOP * ((plane + k) % planes) + 1 - side
            arrivals[1, k, 0].wait_recv()
            forward(4, k, 0, theirs, tp, along)
            forward(5, k, 0, theirs, tp, partner)
            arrivals[2, k, 1].wait_recv()
            forward(4, k, 1, mine, other, across)
            forward(6, k, 1, mine, other, partner)
            arrivals[1, k, 1].wait_recv()
            forward(5, k, 1, theirs, tp, partner)
            arrivals[2, k, 0].wait_recv()
            forward(6, k, 0, mine, other, partner)
            arrivals[1, k, 2].wait_recv()
        k = step - 2
        if 0 <= k < planes:
            theirs = TOP * ((plane + k) % planes) + 1 - side
            for array in range(2):
                arrivals[4, k, array].wait_recv()
                forward(7, k, array, theirs, other, partner)
        k = step - 3
        if 0 <= k < planes:
            base = TOP * ((plane + k) % planes)
            if k == 0:
                for copy in local + loads:
                    copy.wait()
            for array in range(2):
                for kind in (3, 5, 6, 7):
                    arrivals[kind, k, array].wait_recv()
            inputs = []
            seeds = []
            for s in range(TOP):
                table = jnp.transpose(out_w[base + s])[:slots]
                weight = jnp.where(side == 0, table[:, 0:1], table[:, 1:2])
                inputs.append(wide(out_m[base + s]))
                seeds.append(weight * wide(out_c[base + s]))
                out_seed[base + s] = seeds[s].astype(out.dtype)
            inputs = jnp.concatenate(inputs, axis=0).astype(out.dtype)
            seeds = jnp.concatenate(seeds, axis=0).astype(out.dtype)
            gate_pre = dot(inputs, gate_w[...], 1, 0)
            up_pre = dot(inputs, up_w[...], 1, 0)
            hidden_grad = dot(seeds, down_w[...], 1, 1)
            sig = jax.nn.sigmoid(gate_pre)
            gate_act = gate_pre * sig
            hidden = gate_act * up_pre
            gate_grad = hidden_grad * up_pre * (sig * (1.0 + gate_pre * (1.0 - sig)))
            up_grad = hidden_grad * gate_act
            sums = dot(gate_grad.astype(out.dtype), gate_w[...], 1, 1)
            sums += dot(up_grad.astype(out.dtype), up_w[...], 1, 1)
            for s in range(TOP):
                rows = slice(s * slots, (s + 1) * slots)
                part[k, s] = sums[rows].astype(out.dtype)
                out_hidden[base + s] = hidden[rows].astype(out.dtype)
                out_gate[base + s] = gate_grad[rows].astype(out.dtype)
                out_up[base + s] = up_grad[rows].astype(out.dtype)
            for j in range(2):
                quarter = 2 * (row if j == 0 else 1 - row) + 1 - core
                give(part.at[k, :, :, columns(quarter)], pair_in.at[k, j], j, k, partner)
        k = step - 4
        if 0 <= k < planes:
            for j, quarter in ((0, tp), (1, other)):
                got(j, k)
                pair_sum[k, j] = (
                    wide(part[k, :, :, columns(quarter)]) + wide(pair_in[k, j])
                ).astype(out.dtype)
            give(pair_sum.at[k, 1, :, :, low], in_y.at[k], 2, k, along)
            give(pair_sum.at[k, :, 1 - side, :, high], in_x.at[k], 3, k, across)
        k = step - 5
        if 0 <= k < planes:
            got(2, k)
            sum_y[k] = (wide(pair_sum[k, 0, :, :, low]) + wide(in_y[k])).astype(out.dtype)
            give(sum_y.at[k, 1 - side], last_x.at[k], 4, k, across)
            got(3, k)
            sum_x[k] = (wide(pair_sum[k, :, side, :, high]) + wide(in_x[k])).astype(out.dtype)
            give(sum_x.at[k, 1], last_y.at[k], 5, k, along)
        k = step - 6
        if 0 <= k < planes:
            got(4, k)
            got(5, k)
            total[k, :, low] = (wide(sum_y[k, side]) + wide(last_x[k])).astype(out.dtype)
            total[k, :, high] = (wide(sum_x[k, 0]) + wide(last_y[k])).astype(out.dtype)
            if k > 0:
                to = (TOP * ((plane + k) % planes) + side, tp)
                give(total.at[k], back.at[plane], 6, k, to)
    moe = dot(pick[plane], total[0], 1, 0)
    for k in range(1, planes):
        got(6, k)
        source = (plane + planes - k) % planes
        moe += dot(pick[source], back[source], 1, 0)
    out[:, columns(tp)] = (wide(cot[...]) + moe).astype(out.dtype)
    mine = out.at[:, columns(tp)]
    remote(mine, mine, g_sem.at[0, 0], g_sem.at[1, 0], "along", along)
    remote(mine, mine, g_sem.at[0, 1], g_sem.at[1, 1], "partner", partner)
    arrivals["along"].wait_recv()
    theirs = out.at[:, columns(other)]
    remote(theirs, theirs, g_sem.at[0, 2], g_sem.at[1, 2], "last", partner)
    arrivals["partner"].wait_recv()
    arrivals["last"].wait_recv()
    for copy in copies:
        copy.wait_send()


def exchange(send_m, send_c, send_w, pick, cot, gate_mat, up_mat, down_mat):
    planes, slots, width = send_m.shape
    token_count = cot.shape[0]
    blocks = planes * TOP
    wide_rows = width * lax.axis_size("tp")
    hidden_width = down_mat.shape[0]
    half = width // 2
    dtype = send_m.dtype
    vmem = pl.BlockSpec(memory_space=pltpu.VMEM)
    hbm = pl.BlockSpec(memory_space=pl.ANY)
    rows = jax.ShapeDtypeStruct((blocks, slots, wide_rows), dtype)
    units = jax.ShapeDtypeStruct((blocks, slots, hidden_width), dtype)
    dma = pltpu.SemaphoreType.DMA
    return pl.pallas_call(
        exchange_kernel,
        out_shape=(
            jax.ShapeDtypeStruct((token_count, wide_rows), dtype), rows, rows, units, units, units
        ),
        in_specs=[vmem] * 5 + [hbm] * 3,
        out_specs=(vmem,) * 6,
        scratch_shapes=[
            pltpu.VMEM((blocks, slots, wide_rows), dtype),
            pltpu.VMEM((blocks,) + send_w.shape[1:], send_w.dtype),
            pltpu.VMEM(gate_mat.shape, dtype),
            pltpu.VMEM(up_mat.shape, dtype),
            pltpu.VMEM(down_mat.shape, dtype),
            pltpu.VMEM((planes, TOP, slots, wide_rows), dtype),
            pltpu.VMEM((planes, 2, TOP, slots, width), dtype),
            pltpu.VMEM((planes, 2, TOP, slots, width), dtype),
            pltpu.VMEM((planes, TOP, slots, half), dtype),
            pltpu.VMEM((planes, 2, slots, half), dtype),
            pltpu.VMEM((planes, TOP, slots, half), dtype),
            pltpu.VMEM((planes, 2, slots, half), dtype),
            pltpu.VMEM((planes, slots, half), dtype),
            pltpu.VMEM((planes, slots, half), dtype),
            pltpu.VMEM((planes, slots, width), dtype),
            pltpu.VMEM((planes, slots, width), dtype),
            dma((8, planes, 2)),
            dma((8, planes, 2)),
            dma((2, 2, planes)),
            dma((6,)),
            dma((7, planes)),
            dma((7, planes)),
            dma((2, 3)),
        ],
        compiler_params=pltpu.CompilerParams(
            collective_id=0, has_side_effects=True, vmem_limit_bytes=56 * 1024 * 1024
        ),
        name="exchange",
    )(send_m, send_c, send_w, pick, cot, gate_mat, up_mat, down_mat)


def reduce_kernel(prod, out, in_x, side_sum, in_z, s_sem, r_sem):
    planes = in_x.shape[0]
    plane, side, row, core, across, _, _ = neighbours()
    tp = 2 * row + core
    to = [(TOP * ((plane + k + 1) % planes) + side, tp) for k in range(planes - 1)]
    greet([across] + to)

    def remote(source, target_ref, kind, k, device):
        copy = pltpu.make_async_remote_copy(
            src_ref=source,
            dst_ref=target_ref,
            send_sem=s_sem.at[kind, k],
            recv_sem=r_sem.at[kind, k],
            device_id=device,
            device_id_type=MESH,
        )
        copy.start()
        return copy

    rows_of = [TOP * ((plane + k + 1) % planes) for k in range(planes)]
    crossing = [
        remote(prod.at[rows_of[k] + 1 - side], in_x.at[k], 0, k, across) for k in range(planes)
    ]
    climbing = []
    for k in range(planes):
        crossing[k].wait_recv()
        both = wide(prod[rows_of[k] + side]) + wide(in_x[k])
        if k < planes - 1:
            side_sum[k] = both.astype(prod.dtype)
            climbing.append(remote(side_sum.at[k], in_z.at[k], 1, k, to[k]))
    for k in range(planes - 1):
        climbing[k].wait_recv()
        both += wide(in_z[k])
    out[...] = both
    for copy in crossing + climbing:
        copy.wait_send()


def reduce_rows(prod):
    blocks, rows, width = prod.shape
    planes = blocks // TOP
    vmem = pl.BlockSpec(memory_space=pltpu.VMEM)
    return pl.pallas_call(
        reduce_kernel,
        out_shape=jax.ShapeDtypeStruct((rows, width), jnp.float32),
        in_specs=[vmem],
        out_specs=vmem,
        scratch_shapes=[
            pltpu.VMEM((planes, rows, width), prod.dtype),
            pltpu.VMEM((planes - 1, rows, width), prod.dtype),
            pltpu.VMEM((planes - 1, rows, width), prod.dtype),
            pltpu.SemaphoreType.DMA((2, planes)),
            pltpu.SemaphoreType.DMA((2, planes)),
        ],
        compiler_params=pltpu.CompilerParams(
            collective_id=2, has_side_effects=True, vmem_limit_bytes=32 * 1024 * 1024
        ),
        name="reduce_rows",
    )(prod)


def dot(left, right, left_dim, right_dim):
    return lax.dot_general(
        left, right, (((left_dim,), (right_dim,)), ((), ())), preferred_element_type=jnp.float32
    )


def paired_body(
    mid_state,
    conv_pre,
    conv_taps,
    out_proj,
    route_expert,
    route_weight,
    gate_w,
    up_w,
    down_w,
    cotangent,
):
    experts = lax.axis_size("sp")
    tp_count = lax.axis_size("tp")
    token_count = mid_state.shape[0]
    slot_count = 17 * token_count * TOP // (16 * experts)
    slots = (slot_count + 7) // 8 * 8
    width = D // tp_count
    tp = lax.axis_index("tp")

    group = route_expert[:, 0] // TOP
    in_group = group[None, :] == jnp.arange(GROUPS, dtype=jnp.int32)[:, None]
    positions = jnp.arange(token_count, dtype=jnp.int32)
    earlier = (positions[:, None] < positions[None, :]).astype(jnp.bfloat16)
    ranks = dot(in_group.astype(jnp.bfloat16), earlier, 1, 0)
    rank = jnp.sum(jnp.where(in_group, ranks, 0.0), axis=0).astype(jnp.int32)
    slot = jnp.where(rank < slot_count, group * slots + rank, -1)
    taken = slot[None, :] == jnp.arange(GROUPS * slots, dtype=jnp.int32)[:, None]
    pick = taken.astype(jnp.bfloat16)
    own_state = lax.dynamic_slice_in_dim(mid_state, tp * width, width, 1)
    own_cot = lax.dynamic_slice_in_dim(cotangent, tp * width, width, 1)
    send_m = dot(pick, own_state, 1, 0).astype(jnp.bfloat16).reshape(GROUPS, slots, width)
    send_c = dot(pick, own_cot, 1, 0).astype(jnp.bfloat16).reshape(GROUPS, slots, width)
    swapped = (route_expert[:, 0] % TOP) != 0
    first = jnp.where(swapped, route_weight[:, 1], route_weight[:, 0])
    second = jnp.where(swapped, route_weight[:, 0], route_weight[:, 1])
    slot_weights = [
        jnp.sum(jnp.where(taken, each[None, :], 0.0), axis=1).reshape(GROUPS, 1, slots)
        for each in (first, second)
    ]
    send_w = jnp.pad(
        jnp.concatenate(slot_weights, axis=1), ((0, 0), (0, 8 - TOP), (0, -slots % 128))
    )
    own_slot = slot[None, :, None] == (
        slots * jnp.arange(GROUPS, dtype=jnp.int32)[:, None, None]
        + jnp.arange(slots, dtype=jnp.int32)[None, None, :]
    )
    mid_grad, inputs, seeds, hidden, gate_grad, up_grad = exchange(
        send_m, send_c, send_w, own_slot.astype(jnp.bfloat16), own_cot, gate_w[0], up_w[0], down_w[0]
    )
    inputs, seeds, hidden, gate_grad, up_grad = (
        each.reshape(experts * slots, -1) for each in (inputs, seeds, hidden, gate_grad, up_grad)
    )
    grad_down = dot(hidden, seeds, 0, 0).astype(jnp.bfloat16)
    grad_gate = dot(inputs, gate_grad, 0, 0).astype(jnp.bfloat16)
    grad_up = dot(inputs, up_grad, 0, 0).astype(jnp.bfloat16)
    pre_float = conv_pre.astype(jnp.float32)
    activated = jax.nn.silu(pre_float).astype(jnp.bfloat16)
    mixed_grad = dot(mid_grad, out_proj, 1, 1)
    conv_grad = (mixed_grad * silu_slope(pre_float)).astype(jnp.bfloat16)
    next_head = passed_along(conv_grad[: KERNEL - 1], "sp", -1)
    extended = jnp.concatenate([conv_grad, next_head], axis=0).astype(jnp.float32)
    conv_input_grad = jnp.zeros(conv_grad.shape, jnp.float32)
    for lag_index in range(KERNEL):
        conv_input_grad = (
            conv_input_grad
            + conv_taps[lag_index].astype(jnp.float32)[None, :]
            * extended[lag_index : lag_index + token_count]
        )
    grad_proj = reduce_rows(
        dot(mid_grad, activated, 0, 0).astype(jnp.bfloat16).reshape(experts, D // experts, -1)
    )
    return (grad_gate[None], grad_up[None], grad_down[None], grad_proj, conv_input_grad)


def solution(mesh):
    placed = (
        P("sp", None),
        P("sp", "tp"),
        P(None, "tp"),
        P("tp", None),
        P("sp", None),
        P("sp", None),
        P("sp", None, "tp"),
        P("sp", None, "tp"),
        P("sp", "tp", None),
        P("sp", None),
    )
    experts = mesh.shape["sp"]
    paired = experts == GROUPS * TOP and mesh.shape["tp"] == 4
    return jax.shard_map(
        paired_body if paired else body,
        mesh=mesh,
        in_specs=placed,
        out_specs=(
            P("sp", None, "tp"),
            P("sp", None, "tp"),
            P("sp", "tp", None),
            P("sp", "tp"),
            P("sp", "tp"),
        ),
        check_vma=False,
    )
```

```python
import jax
import jax.numpy as jnp
from jax import lax
from jax.experimental import pallas as pl
from jax.experimental.pallas import tpu as pltpu
from jax.sharding import PartitionSpec as P

D = 2048
KERNEL = 31
TOP = 2
GROUPS = 4
MESH = pl.DeviceIdType.MESH


def passed_along(value, axis, steps):
    count = lax.axis_size(axis)
    initial, last = (max(0, -steps), min(count, count - steps))
    return lax.ppermute(value, axis, [(source, source + steps) for source in range(initial, last)])


def silu_slope(value):
    sig = jax.nn.sigmoid(value)
    return sig * (1.0 + value * (1.0 - sig))


def body(
    mid_state,
    conv_pre,
    conv_taps,
    out_proj,
    route_expert,
    route_weight,
    gate_w,
    up_w,
    down_w,
    cotangent,
):
    groups = lax.axis_size("sp")
    token_count = mid_state.shape[0]
    slot_count = 17 * token_count * TOP // (16 * groups)
    flat_routes = route_expert.reshape(-1)
    one_hot_table = (flat_routes[:, None] == jnp.arange(groups, dtype=jnp.int32)[None, :]).astype(
        jnp.int32
    )
    slot_rank = jnp.sum(jnp.cumsum(one_hot_table, axis=0) * one_hot_table, axis=1) - 1
    kept_mask = slot_rank < slot_count
    slot_index = jnp.where(kept_mask, flat_routes * slot_count + slot_rank, groups * slot_count)
    token_ids = jnp.arange(token_count * TOP, dtype=jnp.int32) // TOP
    route_cot = (
        route_weight.reshape(-1)[:, None] * cotangent[token_ids].astype(jnp.float32)
    ).astype(jnp.bfloat16)
    send_inputs = (
        jnp.zeros((groups * slot_count, D), jnp.bfloat16)
        .at[slot_index]
        .set(mid_state[token_ids], mode="drop")
        .reshape(groups, slot_count, D)
    )
    send_seeds = (
        jnp.zeros((groups * slot_count, D), jnp.bfloat16)
        .at[slot_index]
        .set(route_cot, mode="drop")
        .reshape(groups, slot_count, D)
    )
    got_inputs, got_seeds = (
        lax.all_to_all(send_inputs, "sp", split_axis=0, concat_axis=0, tiled=True),
        lax.all_to_all(send_seeds, "sp", split_axis=0, concat_axis=0, tiled=True),
    )
    inputs = got_inputs.reshape(groups * slot_count, D)
    seeds = got_seeds.reshape(groups * slot_count, D)
    gate_mat = gate_w[0]
    up_mat = up_w[0]
    down_mat = down_w[0]
    gate_pre = jnp.dot(inputs, gate_mat, preferred_element_type=jnp.float32)
    up_pre = jnp.dot(inputs, up_mat, preferred_element_type=jnp.float32)
    gate_act = jax.nn.silu(gate_pre)
    hidden = (gate_act * up_pre).astype(jnp.bfloat16)
    hidden_grad = lax.dot_general(
        seeds, down_mat, (((1,), (1,)), ((), ())), preferred_element_type=jnp.float32
    )
    gate_grad = (hidden_grad * up_pre * silu_slope(gate_pre)).astype(jnp.bfloat16)
    up_grad = (hidden_grad * gate_act).astype(jnp.bfloat16)
    grad_down = lax.dot_general(
        hidden, seeds, (((0,), (0,)), ((), ())), preferred_element_type=jnp.float32
    ).astype(jnp.bfloat16)
    grad_gate = lax.dot_general(
        inputs, gate_grad, (((0,), (0,)), ((), ())), preferred_element_type=jnp.float32
    ).astype(jnp.bfloat16)
    grad_up = lax.dot_general(
        inputs, up_grad, (((0,), (0,)), ((), ())), preferred_element_type=jnp.float32
    ).astype(jnp.bfloat16)
    weight_results = (grad_gate, grad_up, grad_down)
    partial_value = lax.dot_general(
        gate_grad, gate_mat, (((1,), (1,)), ((), ())), preferred_element_type=jnp.float32
    )
    partial_value = partial_value + lax.dot_general(
        up_grad, up_mat, (((1,), (1,)), ((), ())), preferred_element_type=jnp.float32
    )
    partial_value = partial_value.astype(jnp.bfloat16).astype(jnp.float32)
    safe_index = jnp.minimum(slot_index, groups * slot_count - 1)
    slice_width = D // lax.axis_size("tp")
    summed = lax.psum_scatter(
        partial_value.astype(jnp.bfloat16), "tp", scatter_dimension=1, tiled=True
    )
    returned = lax.all_to_all(
        summed.reshape(groups, slot_count, slice_width),
        "sp",
        split_axis=0,
        concat_axis=0,
        tiled=True,
    ).reshape(groups * slot_count, slice_width)
    picked = jnp.where(
        kept_mask[:, None], returned[safe_index].astype(jnp.float32), jnp.float32(0.0)
    )
    moe_grad = jnp.sum(picked.reshape(token_count, TOP, slice_width), axis=1)
    own_cot = lax.dynamic_slice_in_dim(
        cotangent, lax.axis_index("tp") * slice_width, slice_width, 1
    )
    mid_part = (own_cot.astype(jnp.float32) + moe_grad).astype(jnp.bfloat16)
    mid_grad = lax.all_gather(mid_part, "tp", axis=1, tiled=True)
    grad_gate, grad_up, grad_down = weight_results
    pre_float = conv_pre.astype(jnp.float32)
    activated = jax.nn.silu(pre_float).astype(jnp.bfloat16)
    mixed_grad = lax.dot_general(
        mid_grad, out_proj, (((1,), (1,)), ((), ())), preferred_element_type=jnp.float32
    )
    conv_grad = (mixed_grad * silu_slope(pre_float)).astype(jnp.bfloat16)
    next_head = passed_along(conv_grad[: KERNEL - 1], "sp", -1)
    extended = jnp.concatenate([conv_grad, next_head], axis=0).astype(jnp.float32)
    conv_input_grad = jnp.zeros(conv_grad.shape, jnp.float32)
    for lag_index in range(KERNEL):
        conv_input_grad = (
            conv_input_grad
            + conv_taps[lag_index].astype(jnp.float32)[None, :]
            * extended[lag_index : lag_index + token_count]
        )
    grad_proj = lax.psum_scatter(
        lax.dot_general(
            mid_grad, activated, (((0,), (0,)), ((), ())), preferred_element_type=jnp.float32
        ).astype(jnp.bfloat16),
        "sp",
        scatter_dimension=0,
        tiled=True,
    ).astype(jnp.float32)
    return (grad_gate[None], grad_up[None], grad_down[None], grad_proj, conv_input_grad)


def neighbours():
    sp, tp = lax.axis_index("sp"), lax.axis_index("tp")
    plane, side = sp // TOP, sp % TOP
    row, core = tp // 2, tp % 2
    across = (TOP * plane + 1 - side, tp)
    along = (sp, 2 * (1 - row) + core)
    partner = (sp, 2 * row + 1 - core)
    return plane, side, row, core, across, along, partner


def greet(targets):
    barrier = pltpu.get_barrier_semaphore()
    for target in targets:
        pl.semaphore_signal(barrier, inc=1, device_id=target, device_id_type=MESH)
    pl.semaphore_wait(barrier, len(targets))


def wide(value):
    return value.astype(jnp.float32)


def exchange_kernel(
    send_m, send_c, send_w, pick, cot, gate_hbm, up_hbm, down_hbm,
    out, out_m, out_seed, out_hidden, out_gate, out_up,
    out_c, out_w, gate_w, up_w, down_w, part,
    pair_in, pair_sum, in_y, in_x, sum_y, sum_x, last_x, last_y, total, back,
    s_sem, r_sem, w_sem, l_sem, s2_sem, r2_sem, g_sem
):
    planes, slots, width = send_m.shape
    half = width // 2
    plane, side, row, core, across, along, partner = neighbours()
    own = TOP * plane + side
    tp = 2 * row + core
    other = 2 * (1 - row) + core
    sends = (send_m, send_c)
    outs = (out_m, out_c)

    loads = [
        pltpu.make_async_copy(source, target, l_sem.at[3 + i])
        for i, (source, target) in enumerate(
            ((gate_hbm, gate_w), (up_hbm, up_w), (down_hbm, down_w))
        )
    ]
    for load in loads:
        load.start()
    greet(
        [across, along, partner]
        + [(TOP * ((plane + k) % planes) + side, tp) for k in range(1, planes)]
    )
    copies = []
    arrivals = {}

    def columns(quarter):
        return pl.ds(pl.multiple_of(quarter * width, width), width)

    def place(array, block, quarter):
        return outs[array].at[block, :, columns(quarter)]

    def remote(source, target_ref, send_sem, recv_sem, key, device):
        copy = pltpu.make_async_remote_copy(
            src_ref=source,
            dst_ref=target_ref,
            send_sem=send_sem,
            recv_sem=recv_sem,
            device_id=device,
            device_id_type=MESH,
        )
        copy.start()
        copies.append(copy)
        arrivals[key] = copy

    def move(source, target_ref, kind, k, array, device):
        remote(
            source, target_ref, s_sem.at[kind, k, array], r_sem.at[kind, k, array],
            (kind, k, array), device,
        )

    def weights(source, block, kind, k, device):
        remote(
            source, out_w.at[block], w_sem.at[0, kind, k], w_sem.at[1, kind, k],
            (kind, k, 2), device,
        )

    def give(source, target_ref, kind, k, device):
        remote(
            source, target_ref, s2_sem.at[kind, k], r2_sem.at[kind, k], ("give", kind, k), device
        )

    def got(kind, k):
        arrivals["give", kind, k].wait_recv()

    for k in range(1, planes):
        to = (plane - k + planes) % planes
        device = (TOP * to + side, tp)
        for array in range(2):
            move(sends[array].at[to], place(array, own, tp), 0, k, array, device)
        weights(send_w.at[to], own, 0, k, device)
    local = [
        pltpu.make_async_copy(sends[array].at[plane], place(array, own, tp), l_sem.at[array])
        for array in range(2)
    ]
    local.append(pltpu.make_async_copy(send_w.at[plane], out_w.at[own], l_sem.at[2]))
    for copy in local:
        copy.start()

    def forward(kind, k, array, block, quarter, device, source=None):
        ref = place(array, block, quarter)
        move(ref if source is None else source, ref, kind, k, array, device)

    low, high = pl.ds(0, half), pl.ds(half, half)
    for step in range(planes + 6):
        k = step
        if k < planes:
            block = TOP * ((plane + k) % planes) + side
            for array in range(2):
                if k > 0:
                    arrivals[0, k, array].wait_recv()
                source = sends[array].at[plane] if k == 0 else None
                forward(1, k, array, block, tp, across, source)
                forward(2, k, array, block, tp, along, source)
                forward(3, k, array, block, tp, partner, source)
            if k > 0:
                arrivals[0, k, 2].wait_recv()
            weights(send_w.at[plane] if k == 0 else out_w.at[block], block, 1, k, across)
        k = step - 1
        if 0 <= k < planes:
            mine = TOP * ((plane + k) % planes) + side
            theirs = TOP * ((plane + k) % planes) + 1 - side
            arrivals[1, k, 0].wait_recv()
            forward(4, k, 0, theirs, tp, along)
            forward(5, k, 0, theirs, tp, partner)
            arrivals[2, k, 1].wait_recv()
            forward(4, k, 1, mine, other, across)
            forward(6, k, 1, mine, other, partner)
            arrivals[1, k, 1].wait_recv()
            forward(5, k, 1, theirs, tp, partner)
            arrivals[2, k, 0].wait_recv()
            forward(6, k, 0, mine, other, partner)
            arrivals[1, k, 2].wait_recv()
        k = step - 2
        if 0 <= k < planes:
            theirs = TOP * ((plane + k) % planes) + 1 - side
            for array in range(2):
                arrivals[4, k, array].wait_recv()
                forward(7, k, array, theirs, other, partner)
        k = step - 3
        if 0 <= k < planes:
            base = TOP * ((plane + k) % planes)
            if k == 0:
                for copy in local + loads:
                    copy.wait()
            for array in range(2):
                for kind in (3, 5, 6, 7):
                    arrivals[kind, k, array].wait_recv()
            inputs = []
            seeds = []
            for s in range(TOP):
                table = jnp.transpose(out_w[base + s])[:slots]
                weight = jnp.where(side == 0, table[:, 0:1], table[:, 1:2])
                inputs.append(wide(out_m[base + s]))
                seeds.append(weight * wide(out_c[base + s]))
                out_seed[base + s] = seeds[s].astype(out.dtype)
            inputs = jnp.concatenate(inputs, axis=0).astype(out.dtype)
            seeds = jnp.concatenate(seeds, axis=0).astype(out.dtype)
            gate_pre = dot(inputs, gate_w[...], 1, 0)
            up_pre = dot(inputs, up_w[...], 1, 0)
            hidden_grad = dot(seeds, down_w[...], 1, 1)
            sig = jax.nn.sigmoid(gate_pre)
            gate_act = gate_pre * sig
            hidden = gate_act * up_pre
            gate_grad = hidden_grad * up_pre * (sig * (1.0 + gate_pre * (1.0 - sig)))
            up_grad = hidden_grad * gate_act
            sums = dot(gate_grad.astype(out.dtype), gate_w[...], 1, 1)
            sums += dot(up_grad.astype(out.dtype), up_w[...], 1, 1)
            for s in range(TOP):
                rows = slice(s * slots, (s + 1) * slots)
                part[k, s] = sums[rows].astype(out.dtype)
                out_hidden[base + s] = hidden[rows].astype(out.dtype)
                out_gate[base + s] = gate_grad[rows].astype(out.dtype)
                out_up[base + s] = up_grad[rows].astype(out.dtype)
            for j in range(2):
                quarter = 2 * (row if j == 0 else 1 - row) + 1 - core
                give(part.at[k, :, :, columns(quarter)], pair_in.at[k, j], j, k, partner)
        k = step - 4
        if 0 <= k < planes:
            for j, quarter in ((0, tp), (1, other)):
                got(j, k)
                pair_sum[k, j] = (
                    wide(part[k, :, :, columns(quarter)]) + wide(pair_in[k, j])
                ).astype(out.dtype)
            give(pair_sum.at[k, 1, :, :, low], in_y.at[k], 2, k, along)
            give(pair_sum.at[k, :, 1 - side, :, high], in_x.at[k], 3, k, across)
        k = step - 5
        if 0 <= k < planes:
            got(2, k)
            sum_y[k] = (wide(pair_sum[k, 0, :, :, low]) + wide(in_y[k])).astype(out.dtype)
            give(sum_y.at[k, 1 - side], last_x.at[k], 4, k, across)
            got(3, k)
            sum_x[k] = (wide(pair_sum[k, :, side, :, high]) + wide(in_x[k])).astype(out.dtype)
            give(sum_x.at[k, 1], last_y.at[k], 5, k, along)
        k = step - 6
        if 0 <= k < planes:
            got(4, k)
            got(5, k)
            total[k, :, low] = (wide(sum_y[k, side]) + wide(last_x[k])).astype(out.dtype)
            total[k, :, high] = (wide(sum_x[k, 0]) + wide(last_y[k])).astype(out.dtype)
            if k > 0:
                to = (TOP * ((plane + k) % planes) + side, tp)
                give(total.at[k], back.at[plane], 6, k, to)
    moe = dot(pick[plane], total[0], 1, 0)
    for k in range(1, planes):
        got(6, k)
        source = (plane + planes - k) % planes
        moe += dot(pick[source], back[source], 1, 0)
    out[:, columns(tp)] = (wide(cot[...]) + moe).astype(out.dtype)
    mine = out.at[:, columns(tp)]
    remote(mine, mine, g_sem.at[0, 0], g_sem.at[1, 0], "along", along)
    remote(mine, mine, g_sem.at[0, 1], g_sem.at[1, 1], "partner", partner)
    arrivals["along"].wait_recv()
    theirs = out.at[:, columns(other)]
    remote(theirs, theirs, g_sem.at[0, 2], g_sem.at[1, 2], "last", partner)
    arrivals["partner"].wait_recv()
    arrivals["last"].wait_recv()
    for copy in copies:
        copy.wait_send()


def exchange(send_m, send_c, send_w, pick, cot, gate_mat, up_mat, down_mat):
    planes, slots, width = send_m.shape
    token_count = cot.shape[0]
    blocks = planes * TOP
    wide_rows = width * lax.axis_size("tp")
    hidden_width = down_mat.shape[0]
    half = width // 2
    dtype = send_m.dtype
    vmem = pl.BlockSpec(memory_space=pltpu.VMEM)
    hbm = pl.BlockSpec(memory_space=pl.ANY)
    rows = jax.ShapeDtypeStruct((blocks, slots, wide_rows), dtype)
    units = jax.ShapeDtypeStruct((blocks, slots, hidden_width), dtype)
    dma = pltpu.SemaphoreType.DMA
    return pl.pallas_call(
        exchange_kernel,
        out_shape=(
            jax.ShapeDtypeStruct((token_count, wide_rows), dtype), rows, rows, units, units, units
        ),
        in_specs=[vmem] * 5 + [hbm] * 3,
        out_specs=(vmem,) * 6,
        scratch_shapes=[
            pltpu.VMEM((blocks, slots, wide_rows), dtype),
            pltpu.VMEM((blocks,) + send_w.shape[1:], send_w.dtype),
            pltpu.VMEM(gate_mat.shape, dtype),
            pltpu.VMEM(up_mat.shape, dtype),
            pltpu.VMEM(down_mat.shape, dtype),
            pltpu.VMEM((planes, TOP, slots, wide_rows), dtype),
            pltpu.VMEM((planes, 2, TOP, slots, width), dtype),
            pltpu.VMEM((planes, 2, TOP, slots, width), dtype),
            pltpu.VMEM((planes, TOP, slots, half), dtype),
            pltpu.VMEM((planes, 2, slots, half), dtype),
            pltpu.VMEM((planes, TOP, slots, half), dtype),
            pltpu.VMEM((planes, 2, slots, half), dtype),
            pltpu.VMEM((planes, slots, half), dtype),
            pltpu.VMEM((planes, slots, half), dtype),
            pltpu.VMEM((planes, slots, width), dtype),
            pltpu.VMEM((planes, slots, width), dtype),
            dma((8, planes, 2)),
            dma((8, planes, 2)),
            dma((2, 2, planes)),
            dma((6,)),
            dma((7, planes)),
            dma((7, planes)),
            dma((2, 3)),
        ],
        compiler_params=pltpu.CompilerParams(
            collective_id=0, has_side_effects=True, vmem_limit_bytes=56 * 1024 * 1024
        ),
        name="exchange",
    )(send_m, send_c, send_w, pick, cot, gate_mat, up_mat, down_mat)


def reduce_kernel(kept, crossed, out, side_sum, in_z, s_sem, r_sem):
    planes = kept.shape[0]
    plane, side, row, core, _, _, _ = neighbours()
    tp = 2 * row + core
    to = [(TOP * ((plane + k + 1) % planes) + side, tp) for k in range(planes - 1)]
    greet(to)

    def remote(source, target_ref, k, device):
        copy = pltpu.make_async_remote_copy(
            src_ref=source,
            dst_ref=target_ref,
            send_sem=s_sem.at[k],
            recv_sem=r_sem.at[k],
            device_id=device,
            device_id_type=MESH,
        )
        copy.start()
        return copy

    climbing = []
    for k in range(planes - 1):
        at = (plane + k + 1) % planes
        side_sum[k] = (wide(kept[at]) + wide(crossed[at])).astype(kept.dtype)
        climbing.append(remote(side_sum.at[k], in_z.at[k], k, to[k]))
    both = wide(kept[plane]) + wide(crossed[plane])
    for k in range(planes - 1):
        climbing[k].wait_recv()
        both += wide(in_z[k])
    out[...] = both
    for copy in climbing:
        copy.wait_send()


def reduce_rows(kept, crossed):
    planes, rows, width = kept.shape
    vmem = pl.BlockSpec(memory_space=pltpu.VMEM)
    return pl.pallas_call(
        reduce_kernel,
        out_shape=jax.ShapeDtypeStruct((rows, width), jnp.float32),
        in_specs=[vmem, vmem],
        out_specs=vmem,
        scratch_shapes=[
            pltpu.VMEM((planes - 1, rows, width), kept.dtype),
            pltpu.VMEM((planes - 1, rows, width), kept.dtype),
            pltpu.SemaphoreType.DMA((planes,)),
            pltpu.SemaphoreType.DMA((planes,)),
        ],
        compiler_params=pltpu.CompilerParams(
            collective_id=2, has_side_effects=True, vmem_limit_bytes=32 * 1024 * 1024
        ),
        name="reduce_rows",
    )(kept, crossed)


def dot(left, right, left_dim, right_dim):
    return lax.dot_general(
        left, right, (((left_dim,), (right_dim,)), ((), ())), preferred_element_type=jnp.float32
    )


def paired_body(
    mid_state,
    conv_pre,
    conv_taps,
    out_proj,
    route_expert,
    route_weight,
    gate_w,
    up_w,
    down_w,
    cotangent,
):
    experts = lax.axis_size("sp")
    tp_count = lax.axis_size("tp")
    token_count = mid_state.shape[0]
    slot_count = 17 * token_count * TOP // (16 * experts)
    slots = (slot_count + 7) // 8 * 8
    width = D // tp_count
    tp = lax.axis_index("tp")

    group = route_expert[:, 0] // TOP
    in_group = group[None, :] == jnp.arange(GROUPS, dtype=jnp.int32)[:, None]
    positions = jnp.arange(token_count, dtype=jnp.int32)
    earlier = (positions[:, None] < positions[None, :]).astype(jnp.bfloat16)
    ranks = dot(in_group.astype(jnp.bfloat16), earlier, 1, 0)
    rank = jnp.sum(jnp.where(in_group, ranks, 0.0), axis=0).astype(jnp.int32)
    slot = jnp.where(rank < slot_count, group * slots + rank, -1)
    taken = slot[None, :] == jnp.arange(GROUPS * slots, dtype=jnp.int32)[:, None]
    pick = taken.astype(jnp.bfloat16)
    own_state = lax.dynamic_slice_in_dim(mid_state, tp * width, width, 1)
    own_cot = lax.dynamic_slice_in_dim(cotangent, tp * width, width, 1)
    send_m = dot(pick, own_state, 1, 0).astype(jnp.bfloat16).reshape(GROUPS, slots, width)
    send_c = dot(pick, own_cot, 1, 0).astype(jnp.bfloat16).reshape(GROUPS, slots, width)
    swapped = (route_expert[:, 0] % TOP) != 0
    first = jnp.where(swapped, route_weight[:, 1], route_weight[:, 0])
    second = jnp.where(swapped, route_weight[:, 0], route_weight[:, 1])
    slot_weights = [
        jnp.sum(jnp.where(taken, each[None, :], 0.0), axis=1).reshape(GROUPS, 1, slots)
        for each in (first, second)
    ]
    send_w = jnp.pad(
        jnp.concatenate(slot_weights, axis=1), ((0, 0), (0, 8 - TOP), (0, -slots % 128))
    )
    own_slot = slot[None, :, None] == (
        slots * jnp.arange(GROUPS, dtype=jnp.int32)[:, None, None]
        + jnp.arange(slots, dtype=jnp.int32)[None, None, :]
    )
    mid_grad, inputs, seeds, hidden, gate_grad, up_grad = exchange(
        send_m, send_c, send_w, own_slot.astype(jnp.bfloat16), own_cot, gate_w[0], up_w[0], down_w[0]
    )
    inputs, seeds, hidden, gate_grad, up_grad = (
        each.reshape(experts * slots, -1) for each in (inputs, seeds, hidden, gate_grad, up_grad)
    )
    grad_down = dot(hidden, seeds, 0, 0).astype(jnp.bfloat16)
    grad_gate = dot(inputs, gate_grad, 0, 0).astype(jnp.bfloat16)
    grad_up = dot(inputs, up_grad, 0, 0).astype(jnp.bfloat16)
    pre_float = conv_pre.astype(jnp.float32)
    activated = jax.nn.silu(pre_float).astype(jnp.bfloat16)
    mixed_grad = dot(mid_grad, out_proj, 1, 1)
    conv_grad = (mixed_grad * silu_slope(pre_float)).astype(jnp.bfloat16)
    next_head = passed_along(conv_grad[: KERNEL - 1], "sp", -1)
    extended = jnp.concatenate([conv_grad, next_head], axis=0).astype(jnp.float32)
    conv_input_grad = jnp.zeros(conv_grad.shape, jnp.float32)
    for lag_index in range(KERNEL):
        conv_input_grad = (
            conv_input_grad
            + conv_taps[lag_index].astype(jnp.float32)[None, :]
            * extended[lag_index : lag_index + token_count]
        )
    prod = dot(mid_grad, activated, 0, 0).astype(jnp.bfloat16)
    prod = prod.reshape(experts // TOP, TOP, D // experts, -1)
    side = lax.axis_index("sp") % TOP
    kept = lax.dynamic_index_in_dim(prod, side, 1, keepdims=False)
    crossing = lax.dynamic_index_in_dim(prod, 1 - side, 1, keepdims=False)
    crossed = lax.ppermute(crossing, "sp", [(i, i + 1 - 2 * (i % TOP)) for i in range(experts)])
    grad_proj = reduce_rows(kept, crossed)
    return (grad_gate[None], grad_up[None], grad_down[None], grad_proj, conv_input_grad)


def solution(mesh):
    placed = (
        P("sp", None),
        P("sp", "tp"),
        P(None, "tp"),
        P("tp", None),
        P("sp", None),
        P("sp", None),
        P("sp", None, "tp"),
        P("sp", None, "tp"),
        P("sp", "tp", None),
        P("sp", None),
    )
    experts = mesh.shape["sp"]
    paired = experts == GROUPS * TOP and mesh.shape["tp"] == 4
    return jax.shard_map(
        paired_body if paired else body,
        mesh=mesh,
        in_specs=placed,
        out_specs=(
            P("sp", None, "tp"),
            P("sp", None, "tp"),
            P("sp", "tp", None),
            P("sp", "tp"),
            P("sp", "tp"),
        ),
        check_vma=False,
    )
```
